32 devices in a mesh: sp: 8 (over z, x), tp: 4 (over y, core).
Axes of the slice: x: 2, y: 2, z: 4, core: 2. Of those that a mesh axis runs over, the one named last changes fastest.
Arguments:
- moe_input: bfloat16 [1536, 2048], P('sp'), may hold values from -6 to 6
- out_grad: bfloat16 [1536, 2048], P('sp', 'tp'), may hold values from -6 to 6
- expert_ids: int32 [1536, 2], P('sp'), may hold values from 0 to 7, all different within a row; in each aligned block of 192 rows (0 to 191, 192 to 383, ...) at most 60 rows name the same one
- expert_weights: float32 [1536, 2], P('sp'), may hold values from 0.1 to 0.9
- w_gate: bfloat16 [8, 2048, 2048], P('sp', None, 'tp'), may hold values from -0.125 to 0.125
- w_up: bfloat16 [8, 2048, 2048], P('sp', None, 'tp'), may hold values from -0.125 to 0.125
- w_down: bfloat16 [8, 2048, 2048], P('sp', 'tp'), may hold values from -0.125 to 0.125
- out_proj: bfloat16 [1536, 2048], P('tp'), may hold values from -0.15625 to 0.15625
- retained: bfloat16 [1536, 1536], P('sp', 'tp'), may hold values from -6 to 6
- queries: bfloat16 [1536, 768], P('sp', 'tp'), may hold values from -6 to 6
- keys: bfloat16 [1536, 768], P('sp', 'tp'), may hold values from -0.86328125 to 0.86328125
- values: bfloat16 [1536, 1536], P('sp', 'tp'), may hold values from -6 to 6
- log_decay: float32 [1536, 16], P('sp', 'tp'), may hold values from -1 to 0
- incoming_state: float32 [8, 16, 48, 96], P('sp', 'tp'), may hold values from -6 to 6
Outputs:
- w_gate_grad: bfloat16 [8, 2048, 2048], P('sp', None, 'tp')
- w_up_grad: bfloat16 [8, 2048, 2048], P('sp', None, 'tp')
- w_down_grad: bfloat16 [8, 2048, 2048], P('sp', 'tp')
- out_proj_grad: float32 [2048, 1536], P('sp', 'tp')
- query_grad: bfloat16 [1536, 768], P('sp', 'tp')
- key_grad: bfloat16 [1536, 768], P('sp', 'tp')
- value_grad: bfloat16 [1536, 1536], P('sp', 'tp')
The draws below stay inside these ranges and needn't reach their ends.
Inputs may be any that keep to these rules, and one draw needn't show every extreme that they name: `expert_ids`: in each aligned block of 192 positions no expert is named by more than 60 of the block's assignments, a bound that some block reaches.
All inputs are finite; a program needn't handle non-finite values.
Results may differ from the reference program's by a relative error of at most 0.02.
Values may be sent and summed in bfloat16 or wider, within the bound.
A program may use at most 64 MiB of HBM per device.

```python
import math
import jax
import jax.numpy as jnp
import numpy as np
from jax import lax

D = 2048
RETENTION_HEADS = 16
KEY_DIM = 48
VALUE_DIM = 96
FF = 2048
TOK_DEV = 192
SEQUENCE_TOKENS = 1536
EXPERTS = 8
CAP = 60
RET_WIDTH = 1536
KEY_WIDTH = 768
N_SP = 8
N_TP = 4


def draw_log_decay(key, part):
    keys = jax.random.split(jax.random.fold_in(key, 17), 7)
    slow_share = 0.5
    slow = jax.random.uniform(keys[0], (RETENTION_HEADS,), jnp.float32) < slow_share
    slow_rate = jnp.exp(jax.random.uniform(keys[1], (RETENTION_HEADS,), jnp.float32, jnp.log(0.1), jnp.log(0.6))) / SEQUENCE_TOKENS
    fast_rate = jax.random.uniform(keys[2], (RETENTION_HEADS,), jnp.float32, 1.0 / 50.0, 1.0 / 30.0)
    decay_rate = jnp.where(slow, slow_rate, fast_rate)
    block_multiplier = jnp.repeat(jax.random.uniform(keys[3], (SEQUENCE_TOKENS // TOK_DEV,), jnp.float32, 0.5, 1.6), TOK_DEV)
    coarse_estimate = jax.random.uniform(keys[4], (SEQUENCE_TOKENS, 1), jnp.float32, 0.5, 1.5)
    spike_position = jax.random.randint(keys[5], (3,), 0, SEQUENCE_TOKENS)
    spike_mask = jnp.any(jnp.arange(SEQUENCE_TOKENS)[:, None] == spike_position[None, :], axis=1).astype(jnp.float32)
    spike_length = jax.random.uniform(keys[6], (RETENTION_HEADS,), jnp.float32, 0.22, 0.51)
    return -(decay_rate[None, :] * block_multiplier[:, None] * coarse_estimate) - spike_mask[:, None] * spike_length[None, :]


def raised(drawn, rng, source, target, blocks, factor):
    owner, partner = [(jnp.arange(drawn.shape[axis_at]) // (drawn.shape[axis_at] // blocks)).reshape([-1 if axis == axis_at else 1 for axis in range(drawn.ndim)]) for axis_at in (source, target)]
    chosen = jax.random.permutation(rng, blocks)[partner]
    strong = (owner == chosen) | (owner == (partner + blocks // 2) % blocks)
    return jnp.where(strong, factor * drawn, drawn)


def block_scale(key, shape, pieces, smallest, high):
    def one(position, blocks):
        heights = jax.random.uniform(jax.random.fold_in(jax.random.fold_in(key, 6), position), (blocks,), jnp.float32, smallest / len(pieces), high / len(pieces))
        return jnp.repeat(jnp.exp(heights), shape[position] // blocks).reshape((-1,) + (1,) * (len(shape) - position - 1))

    gain = one(*pieces[0])
    for cut in pieces[1:]:
        gain = gain * one(*cut)
    return gain


def deal_out(rng, own, number, rows, number_of, top, bound, slope):
    sequence = jax.random.permutation(rng, number_of)
    crowded, usual = load_shares(number_of, rows * top, bound, slope, True), load_shares(number_of, rows * top, bound, slope, False)
    places = jnp.arange(number_of)

    def named(tallies, rotation):
        used = int((tallies > 0).sum())
        fixed = max(1, used // 4)
        moved = fixed + (places - fixed + rotation * (used - fixed)) % max(1, number_of - fixed)
        return jnp.zeros((number_of,), jnp.int32).at[sequence[jnp.where(places < fixed, places, moved)]].set(jnp.asarray(tallies, jnp.int32))

    tallies = jnp.where(number % 4 == 0, named(crowded, number // 4), named(usual, number - number // 4 - 1))
    mixed = jax.random.permutation(jax.random.fold_in(own, 3), number_of)
    giver, receiver = mixed[0:number_of // 2 * 2:2], mixed[1:number_of // 2 * 2:2]
    slack = jnp.minimum(tallies[giver] - 1, bound - tallies[receiver]) // 2
    slack = jnp.where((giver == sequence[0]) | (receiver == sequence[0]) | (tallies[receiver] == 0), 0, jnp.maximum(slack, 0))
    moved = jax.random.randint(jax.random.fold_in(own, 4), (number_of // 2,), 0, 1 << 20) % (slack + 1)
    tallies = tallies.at[giver].add(-moved).at[receiver].add(moved)
    items = jnp.searchsorted(jnp.cumsum(tallies), jnp.arange(rows * top), side="right").astype(jnp.int32)
    grid = items.reshape(top, rows).T
    grid = grid[jax.random.permutation(jax.random.fold_in(own, 1), rows)]
    rotation = jax.random.randint(jax.random.fold_in(own, 2), (rows, 1), 0, top)
    return jnp.take_along_axis(grid, (jnp.arange(top)[None, :] + rotation) % top, axis=1)


def load_shares(number_of, total, reach, lean, full):
    loads = [(1 << 20) // math.isqrt(grade ** lean) + 1 for grade in range(1, number_of + 1)]
    largest = reach if full else min(reach, max(-(-total // number_of), total * loads[0] // sum(loads)))
    least = 1 if total - largest >= number_of - 1 else 0
    given, spare = [largest] + [least] * (number_of - 1), total - largest - least * (number_of - 1)
    while spare > 0:
        free = [i for i in range(1, number_of) if given[i] < largest] or [i for i in range(1, number_of) if given[i] < reach]
        pool, left = sum([loads[i] for i in free]), spare
        for i in free:
            addition = min(reach - given[i], max(1, left * loads[i] // pool), spare)
            given[i] = given[i] + addition
            spare = spare - addition
    return np.array(given)


def normal_values(key, dims, deviation, bound, cuts=(), kind=jnp.bfloat16):
    drawn = deviation * jax.random.normal(key, dims, jnp.float32)
    if cuts:
        drawn = drawn * block_scale(key, dims, cuts, -0.22, 0.18)
    return jnp.clip(drawn, -bound, bound).astype(kind)


def gaussian_with(key, shape, deviation, reach, cuts, heavy, kind=jnp.bfloat16):
    drawn = deviation * jax.random.normal(key, shape, jnp.float32)
    if cuts:
        drawn = drawn * block_scale(key, shape, cuts, -0.22, 0.18)
    return jnp.clip(raised(drawn, jax.random.fold_in(key, 3), *heavy), -reach, reach).astype(kind)


def setup_inputs(seed: int = 0) -> dict:
    key_list = jax.random.split(jax.random.key(seed), 15)
    moe_input = normal_values(key_list[0], (SEQUENCE_TOKENS, D), 1.0, 6.0, ((0, 8),))
    out_grad = gaussian_with(key_list[1], (SEQUENCE_TOKENS, D), 1.0, 6.0, ((0, 8), (1, 4)), (0, 1, 8, 2.0))
    expert_ids_keys = jax.random.split(jax.random.fold_in(key_list[2], 1), SEQUENCE_TOKENS // TOK_DEV)
    expert_ids_turns = jax.random.permutation(jax.random.fold_in(key_list[2], 3), SEQUENCE_TOKENS // TOK_DEV)
    expert_ids = jax.vmap(lambda own, number: deal_out(jax.random.fold_in(key_list[2], 2), own, number, TOK_DEV, EXPERTS, 2, CAP, 1))(expert_ids_keys, expert_ids_turns).reshape((SEQUENCE_TOKENS, 2))
    expert_weights = jnp.clip(0.1 + 0.79999997 * jax.random.uniform(key_list[3], (SEQUENCE_TOKENS, 2), jnp.float32) ** block_scale(key_list[3], (SEQUENCE_TOKENS, 2), ((0, 8),), -0.2, 0.2), 0.1, 0.9)
    w_gate = normal_values(key_list[4], (EXPERTS, D, FF), D ** -0.5, 0.125, ((0, 8), (2, 4)))
    w_up = normal_values(key_list[5], (EXPERTS, D, FF), D ** -0.5, 0.125, ((0, 8), (2, 4)))
    w_down = normal_values(key_list[6], (EXPERTS, FF, D), FF ** -0.5, 0.125, ((0, 8), (1, 4)))
    out_proj = normal_values(key_list[7], (RET_WIDTH, D), RET_WIDTH ** -0.5, 0.15625, ((0, 4),))
    retained = normal_values(key_list[8], (SEQUENCE_TOKENS, RET_WIDTH), 1.0, 6.0, ((0, 8), (1, 4)))
    queries = normal_values(key_list[9], (SEQUENCE_TOKENS, KEY_WIDTH), 1.0, 6.0, ((0, 8), (1, 4)))
    keys = normal_values(key_list[10], (SEQUENCE_TOKENS, KEY_WIDTH), (KEY_DIM ** -0.5), 0.86328125, ((0, 8), (1, 4)))
    values = normal_values(key_list[11], (SEQUENCE_TOKENS, RET_WIDTH), 1.0, 6.0, ((0, 8), (1, 4)))
    log_decay = draw_log_decay(jax.random.fold_in(key_list[14], 71), 0)
    incoming_state = normal_values(key_list[13], (N_SP, RETENTION_HEADS, KEY_DIM, VALUE_DIM), 1.0, 6.0, ((0, 8), (1, 4)), jnp.float32)
    return dict(moe_input=moe_input, out_grad=out_grad, expert_ids=expert_ids, expert_weights=expert_weights, w_gate=w_gate, w_up=w_up, w_down=w_down, out_proj=out_proj, retained=retained, queries=queries, keys=keys, values=values, log_decay=log_decay, incoming_state=incoming_state)


def slot_table(expert_ids, expert_weights):
    per_block = expert_ids.reshape(N_SP, 2 * TOK_DEV)
    block_weights = expert_weights.reshape(N_SP, 2 * TOK_DEV)
    onehot = (per_block[:, :, None] == jnp.arange(EXPERTS, dtype=jnp.int32)[None, None, :]).astype(jnp.int32)
    ranks = jnp.sum((jnp.cumsum(onehot, axis=1) - onehot) * onehot, axis=2).astype(jnp.int32)
    block = jnp.arange(N_SP, dtype=jnp.int32)[:, None]
    dest = (per_block * (N_SP * CAP) + block * CAP + ranks).reshape(-1).astype(jnp.int32)
    token = (block * TOK_DEV + jnp.arange(2 * TOK_DEV, dtype=jnp.int32)[None, :] // 2).reshape(-1).astype(jnp.int32)
    table = jnp.full((EXPERTS * N_SP * CAP,), SEQUENCE_TOKENS, jnp.int32).at[dest].set(token)
    weight = jnp.zeros((EXPERTS * N_SP * CAP,), jnp.float32).at[dest].set(block_weights.reshape(-1))
    return table.reshape(EXPERTS, N_SP * CAP), weight.reshape(EXPERTS, N_SP * CAP)


def reference(moe_input, out_grad, expert_ids, expert_weights, w_gate, w_up, w_down, out_proj,
              retained, queries, keys, values, log_decay, incoming_state):
    f32 = jnp.float32
    bf16 = jnp.bfloat16
    upper_limit = lax.Precision.HIGHEST
    table, weight = slot_table(expert_ids, expert_weights)
    padded_rows = jnp.concatenate([moe_input, jnp.zeros((1, D), bf16)], axis=0)
    padded_grad = jnp.concatenate([out_grad, jnp.zeros((1, D), bf16)], axis=0)
    part = FF // N_TP

    def expert_back(args):
        index, slot_weight, gate_w, up_w, down_w = args
        rows = padded_rows[index]
        grad = (padded_grad[index].astype(f32) * slot_weight[:, None]).astype(bf16)
        gate = jnp.dot(rows, gate_w, preferred_element_type=f32)
        up = jnp.dot(rows, up_w, preferred_element_type=f32)
        sig = jax.nn.sigmoid(gate)
        swish = gate * sig
        act = (swish * up).astype(bf16)
        act_grad = jnp.dot(grad, down_w.T, preferred_element_type=f32)
        gate_grad = (act_grad * up * sig * (1.0 + gate * (1.0 - sig))).astype(bf16)
        up_grad = (act_grad * swish).astype(bf16)
        down_grad = jnp.dot(act.T, grad, preferred_element_type=f32).astype(bf16)
        gate_w_grad = jnp.dot(rows.T, gate_grad, preferred_element_type=f32).astype(bf16)
        up_w_grad = jnp.dot(rows.T, up_grad, preferred_element_type=f32).astype(bf16)
        slots = rows.shape[0]
        parts = (jnp.einsum('snf,dnf->nsd', gate_grad.astype(f32).reshape(slots, N_TP, part),
                            gate_w.astype(f32).reshape(D, N_TP, part))
                 + jnp.einsum('snf,dnf->nsd', up_grad.astype(f32).reshape(slots, N_TP, part),
                              up_w.astype(f32).reshape(D, N_TP, part)))
        rounded = lax.optimization_barrier(parts.astype(bf16))
        slot_in = jnp.sum(rounded.astype(f32), axis=0).astype(bf16)
        return gate_w_grad, up_w_grad, down_grad, slot_in

    w_gate_grad, w_up_grad, w_down_grad, slot_in = lax.map(expert_back, (table, weight, w_gate, w_up, w_down))
    token_grad = jnp.zeros((SEQUENCE_TOKENS + 1, D), f32).at[table.reshape(-1)].add(
        slot_in.reshape(-1, D).astype(f32))[:SEQUENCE_TOKENS]
    stream = (out_grad.astype(f32) + token_grad).astype(bf16)
    ret_grad = jnp.dot(stream, out_proj.T, preferred_element_type=f32).astype(bf16)
    out_proj_grad = jnp.dot(stream.T, retained, preferred_element_type=f32)

    q = queries.astype(f32).reshape(N_SP, TOK_DEV, RETENTION_HEADS, KEY_DIM)
    k = keys.astype(f32).reshape(N_SP, TOK_DEV, RETENTION_HEADS, KEY_DIM)
    v = values.astype(f32).reshape(N_SP, TOK_DEV, RETENTION_HEADS, VALUE_DIM)
    o = ret_grad.astype(f32).reshape(N_SP, TOK_DEV, RETENTION_HEADS, VALUE_DIM)
    b = jnp.cumsum(log_decay.reshape(N_SP, TOK_DEV, RETENTION_HEADS), axis=1)
    b_end = b[:, -1]
    diff = b[:, :, None, :] - b[:, None, :, :]
    place = jnp.arange(TOK_DEV)
    causal = (place[:, None] >= place[None, :])[None, :, :, None]
    decay = jnp.where(causal, jnp.exp(jnp.minimum(diff, 0.0)), 0.0)
    scores = jnp.einsum('nthk,nshk->ntsh', q, k, precision=upper_limit) * decay
    prob_grad = jnp.einsum('nthv,nshv->ntsh', o, v, precision=upper_limit) * decay
    added_input = jnp.einsum('nth,nthk,nthv->nhkv', jnp.exp(b), q, o, precision=upper_limit)

    def back_step(carry, inputs):
        factor, term = inputs
        return term + factor[:, None, None] * carry, carry

    _, state_gradient = lax.scan(back_step, jnp.zeros((RETENTION_HEADS, KEY_DIM, VALUE_DIM), f32),
                             (jnp.exp(b_end), added_input), reverse=True)
    tail = jnp.exp(b_end[:, None, :] - b)[..., None]
    query_grad = (jnp.einsum('ntsh,nshk->nthk', prob_grad, k, precision=upper_limit)
                  + jnp.exp(b)[..., None] * jnp.einsum('nthv,nhkv->nthk', o, incoming_state, precision=upper_limit))
    key_grad = (jnp.einsum('ntsh,nthk->nshk', prob_grad, q, precision=upper_limit)
                + tail * jnp.einsum('nshv,nhkv->nshk', v, state_gradient, precision=upper_limit))
    value_grad = (jnp.einsum('ntsh,nthv->nshv', scores, o, precision=upper_limit)
                  + tail * jnp.einsum('nshk,nhkv->nshv', k, state_gradient, precision=upper_limit))
    return (w_gate_grad, w_up_grad, w_down_grad, out_proj_grad,
            query_grad.reshape(SEQUENCE_TOKENS, KEY_WIDTH).astype(bf16),
            key_grad.reshape(SEQUENCE_TOKENS, KEY_WIDTH).astype(bf16),
            value_grad.reshape(SEQUENCE_TOKENS, RET_WIDTH).astype(bf16))
```

```python
import functools

import jax
import jax.numpy as jnp
from jax import lax
from jax.experimental import pallas as pl
from jax.experimental.pallas import tpu as pltpu
from jax.sharding import PartitionSpec as P

MESH = pl.DeviceIdType.MESH
F32 = jnp.float32
BF16 = jnp.bfloat16
LIMIT = 60 * 1024 * 1024


def where_am_i(n, ny):
    s, t = lax.axis_index("sp"), lax.axis_index("tp")
    return s, t, lax.div(t, 2), lax.rem(t, 2)


def greet(peers):
    barrier = pltpu.get_barrier_semaphore()
    for peer in peers:
        pl.semaphore_signal(barrier, inc=1, device_id=peer, device_id_type=MESH)
    pl.semaphore_wait(barrier, len(peers))


def sp_peers(n, s, t):
    return [(lax.rem(s + k, n), t) for k in range(1, n)]


def tp_peers(ny, s, y, c):
    return [(s, lax.rem(y + d, ny) * 2 + c) for d in range(1, ny)] + [(s, y * 2 + 1 - c)]


def remote(src, dst, send, recv, peer):
    return pltpu.make_async_remote_copy(
        src_ref=src, dst_ref=dst, send_sem=send, recv_sem=recv, device_id=peer, device_id_type=MESH
    )


def below(a, b, top):
    return lax.div(b - a + top - 1, top)


def nearest_first(z, nz):
    high = nz - 1 - z
    fewer = below(high, z, nz)
    least = z + (high - z) * fewer
    toward = 1 - 2 * fewer
    order = [z]
    for i in range(1, nz):
        both = below(i, 2 * least + 1, 2 * nz)
        step = (i + 1) // 2 * (1 if i % 2 else -1)
        order.append(z + toward * (both * step + (1 - both) * (i - least)))
    return order


def main_kernel(
    n, ny, cap, ids_ref, weights_ref, decay_ref, rows_hbm, grad_ref, kept_ref,
    gate_hbm, up_hbm, down_hbm,
    stream_ref, blocks_ref, kept_out, ends_out, gate_grad_ref, up_grad_ref, down_grad_ref,
    rows_v, gate_w, up_w, down_w, pick, send, slots, act, both_grads, part, near, pairs, far,
    share, back,
    load_sem, a_send, a_recv, e_send, e_recv, y_send, y_recv, p_send, p_recv,
    n_send, n_recv, f_send, f_recv, b_send, b_recv, g_send, g_recv, h_send, h_recv,
    r_send, r_recv, l_send, l_recv, x_send, x_recv,
):
    s, t, y, c = where_am_i(n, ny)
    q = grad_ref.shape[1]
    heads, tokens = decay_ref.shape
    width = gate_w.shape[1]
    nz = n // 2
    z, x = lax.div(s, 2), lax.rem(s, 2)
    partner = (s, y * 2 + 1 - c)
    order = nearest_first(z, nz)
    waits = []

    def columns(tt):
        return pl.ds(pl.multiple_of(tt * q, q), q)

    def block_rows(b):
        return pl.ds(pl.multiple_of(b * cap, cap), cap)

    def chunk_rows(i):
        return pl.ds(pl.multiple_of(order[i] * 2 * cap, 2 * cap), 2 * cap)

    def member(i, e):
        return order[i] * 2 + (x if e == 0 else 1 - x)

    def away(d):
        return (s, lax.rem(y + d, ny) * 2 + c)

    def go(copy, wait):
        copy.start()
        waits.append(getattr(copy, wait))
        return copy

    barrier = pltpu.get_barrier_semaphore()
    peers = sp_peers(n, s, t) + tp_peers(ny, s, y, c)
    for peer in peers:
        pl.semaphore_signal(barrier, inc=1, device_id=peer, device_id_type=MESH)

    own_rows = pltpu.make_async_copy(rows_hbm.at[:, columns(t)], rows_v, load_sem.at[0])
    own_rows.start()
    loads = [
        pltpu.make_async_copy(hbm, local, load_sem.at[1 + j])
        for j, (hbm, local) in enumerate(
            [(gate_hbm.at[0], gate_w), (up_hbm.at[0], up_w), (down_hbm.at[0], down_w)]
        )
    ]
    for copy in loads:
        copy.start()

    ids = ids_ref[...].astype(F32)
    ids = [ids[j : j + 1, :] for j in range(2)]
    weights = [weights_ref[j : j + 1, :] for j in range(2)]
    expert_row = lax.broadcasted_iota(jnp.int32, (n, tokens), 0).astype(F32)
    named = [(expert_row == own).astype(F32) for own in ids]
    first = lax.broadcasted_iota(jnp.int32, (tokens, tokens), 0)
    second = lax.broadcasted_iota(jnp.int32, (tokens, tokens), 1)
    earlier = jnp.dot(
        (named[0] + named[1]).astype(BF16),
        (first < second).astype(F32).astype(BF16),
        preferred_element_type=F32,
    )
    slot = [
        own * cap + jnp.sum(hot * earlier, axis=0, keepdims=True) for own, hot in zip(ids, named)
    ]
    number = lax.broadcasted_iota(jnp.int32, (n * cap, tokens), 0).astype(F32)
    hits = [(number == own).astype(F32) for own in slot]
    picker = (hits[0] + hits[1]).astype(BF16)
    slot_weight = jnp.sum(hits[0] * weights[0] + hits[1] * weights[1], axis=1, keepdims=True)
    pick[...] = picker
    ends_out[s, :, :] = jnp.zeros((8, 128), F32)
    ends_out[s, pl.ds(0, heads), :] = jnp.broadcast_to(
        jnp.sum(decay_ref[...], axis=1, keepdims=True), (heads, 128)
    )
    cotangent = jnp.dot(picker, grad_ref[...], preferred_element_type=F32) * slot_weight
    send[:, 1] = cotangent.astype(BF16).reshape(n, cap, q)
    own_rows.wait()
    picked = jnp.dot(picker, rows_v[...], preferred_element_type=F32).astype(BF16)
    send[:, 0] = picked.reshape(n, cap, q)
    slots[0, block_rows(s), columns(t)] = send[s, 0]
    slots[1, block_rows(s), columns(t)] = send[s, 1]

    pl.semaphore_wait(barrier, len(peers))

    def block(src, tt):
        return slots.at[:, block_rows(src), columns(tt)]

    for i in range(nz):
        for e in range(2):
            if (i, e) != (0, 0):
                to = member(i, e)
                go(
                    remote(send.at[to], block(s, t), a_send.at[2 * i + e], a_recv.at[s], (to, t)),
                    "wait_send",
                )

    def at(zz):
        return lax.rem(zz + 2 * nz, nz) * 2 + x

    def hop(j, sign, send_sem, recv_sem, source):
        held = at(z - sign * j)
        return go(
            remote(
                source, kept_out.at[held], send_sem.at[j], recv_sem.at[j], (at(z + sign), t)
            ),
            "wait_send",
        )

    def across(held, index, source):
        go(
            remote(
                source, kept_out.at[held], x_send.at[index], x_recv.at[index],
                (z * 2 + 1 - x, t),
            ),
            "wait",
        )

    right_steps, left_steps = nz // 2, nz - 1 - nz // 2
    moving = {}

    def kept_start():
        if right_steps:
            moving["right"] = hop(0, 1, r_send, r_recv, kept_ref)
        if left_steps:
            moving["left"] = hop(0, -1, l_send, l_recv, kept_ref)
        across(s, 0, kept_ref)
        kept_out[s] = kept_ref[...]

    def kept_relay(j):
        if j <= right_steps:
            moving["right"].wait_recv()
            held = at(z - j)
            if j < right_steps:
                moving["right"] = hop(j, 1, r_send, r_recv, kept_out.at[held])
            across(held, 2 * j - 1, kept_out.at[held])
        if j <= left_steps:
            moving["left"].wait_recv()
            held = at(z + j)
            if j < left_steps:
                moving["left"] = hop(j, -1, l_send, l_recv, kept_out.at[held])
            across(held, 2 * j, kept_out.at[held])

    from_far, from_partner = {}, {}

    def arrive(i, e):
        src = member(i, e)
        mine = block(src, t)
        if (i, e) != (0, 0):
            remote(
                send.at[src], mine, a_send.at[2 * i + e], a_recv.at[src], (src, t)
            ).wait_recv()
        k = 2 * i + e
        for d in range(1, ny):
            from_far[d, k] = go(
                remote(mine, mine, y_send.at[d, k], y_recv.at[d, k], away(d)), "wait_send"
            )
        from_partner[0, k] = go(
            remote(mine, mine, p_send.at[0, k], p_recv.at[0, k], partner), "wait_send"
        )

    def relay(i, e):
        k = 2 * i + e
        for d in range(1, ny):
            from_far[d, k].wait_recv()
            theirs = block(member(i, e), lax.rem(y - d + ny, ny) * 2 + c)
            from_partner[d, k] = go(
                remote(theirs, theirs, p_send.at[d, k], p_recv.at[d, k], partner), "wait_send"
            )

    across_dims = (((1,), (1,)), ((), ()))
    along_dims = (((0,), (0,)), ((), ()))

    def expert(i):
        for e in range(2):
            for d in range(ny):
                from_partner[d, 2 * i + e].wait_recv()
        r = chunk_rows(i)
        gate = jnp.dot(slots[0, r, :], gate_w[...], preferred_element_type=F32)
        up = jnp.dot(slots[0, r, :], up_w[...], preferred_element_type=F32)
        act_grad = lax.dot_general(
            slots[1, r, :], down_w[...], across_dims, preferred_element_type=F32
        )
        sig = jax.nn.sigmoid(gate)
        swish = gate * sig
        act[r, :] = (swish * up).astype(BF16)
        gate_grad = (act_grad * up * sig * (1.0 + gate * (1.0 - sig))).astype(BF16)
        up_grad = (act_grad * swish).astype(BF16)
        both_grads[r, pl.ds(0, width)] = gate_grad
        both_grads[r, pl.ds(width, width)] = up_grad
        part[r, :] = (
            lax.dot_general(gate_grad, gate_w[...], across_dims, preferred_element_type=F32)
            + lax.dot_general(up_grad, up_w[...], across_dims, preferred_element_type=F32)
        ).astype(BF16)

    halves, summed, returns = {}, {}, {}

    def swap_halves(i):
        r = chunk_rows(i)
        for d in list(range(1, ny)) + [0]:
            theirs = lax.rem(y + d, ny) * 2 + 1 - c
            halves[d, i] = go(
                remote(
                    part.at[r, columns(theirs)], near.at[d, r, :],
                    n_send.at[d, i], n_recv.at[d, i], partner,
                ),
                "wait_send",
            )

    def send_pairs(i):
        r = chunk_rows(i)
        for d in range(1, ny):
            halves[d, i].wait_recv()
            tt = lax.rem(y + d, ny) * 2 + c
            pairs[d, r, :] = (
                part[r, columns(tt)].astype(F32) + near[d, r, :].astype(F32)
            ).astype(BF16)
            summed[d, i] = go(
                remote(
                    pairs.at[d, r, :], far.at[d, r, :], f_send.at[d, i], f_recv.at[d, i], (s, tt)
                ),
                "wait_send",
            )

    def send_back(i):
        r = chunk_rows(i)
        halves[0, i].wait_recv()
        total = part[r, columns(t)].astype(F32) + near[0, r, :].astype(F32)
        for d in range(1, ny):
            summed[d, i].wait_recv()
            total = total + far[d, r, :].astype(F32)
        share[r, :] = total.astype(BF16)
        for e in range(2):
            to = member(i, e)
            if (i, e) == (0, 0):
                back[block_rows(s), :] = share[block_rows(s), :]
            else:
                go(
                    remote(
                        share.at[block_rows(to), :], back.at[block_rows(s), :],
                        b_send.at[2 * i + e], b_recv.at[s], (to, t),
                    ),
                    "wait_send",
                )

    def returned(i):
        for e in range(2):
            if (i, e) != (0, 0):
                src = member(i, e)
                remote(
                    share.at[block_rows(src), :], back.at[block_rows(src), :],
                    b_send.at[2 * i + e], b_recv.at[src], (src, t),
                ).wait_recv()
        r = chunk_rows(i)
        return lax.dot_general(
            pick[r, :], back[r, :], along_dims, preferred_element_type=F32
        )

    def down_grads():
        turned = act[...].T
        wide = 512
        for j in range(0, down_grad_ref.shape[2], wide):
            down_grad_ref[0, :, j : j + wide] = jnp.dot(
                turned, slots[1, :, j : j + wide], preferred_element_type=F32
            ).astype(BF16)

    def in_grads(lo, hi):
        tall = 256

        def step(j, carry):
            band = pl.ds(pl.multiple_of(j * tall, tall), tall)
            grads = lax.dot_general(
                slots[0, :, band], both_grads[...], along_dims, preferred_element_type=F32
            ).astype(BF16)
            gate_grad_ref[0, band, :] = grads[:, :width]
            up_grad_ref[0, band, :] = grads[:, width:]
            return carry

        count = gate_grad_ref.shape[1] // tall
        lax.fori_loop(lo * count // 4, hi * count // 4, step, 0)

    for k in range(1, n):
        to = lax.rem(s + k, n)
        go(remote(ends_out.at[s], ends_out.at[s], e_send.at[k], e_recv.at[k], (to, t)), "wait")
    kept_start()
    for i in range(nz + 1):
        if i < nz:
            arrive(i, 0)
            arrive(i, 1)
        if i == 1:
            for copy in loads:
                copy.wait()
        if i >= 1:
            relay(i - 1, 0)
            relay(i - 1, 1)
        if i >= 2:
            send_pairs(i - 2)
        if i >= 3:
            send_back(i - 3)
        if i >= 1:
            expert(i - 1)
            swap_halves(i - 1)
        if i >= 2:
            kept_relay(i - 1)
    send_back(nz - 2) if nz > 1 else None
    send_pairs(nz - 1)
    down_grads()
    send_back(nz - 1)
    in_grads(0, 2)
    token = returned(0)
    for i in range(1, nz):
        token = token + returned(i)
    stream_ref[:, columns(t)] = (grad_ref[...].astype(F32) + token).astype(BF16)
    mine = stream_ref.at[:, columns(t)]
    outer = {}
    for d in range(1, ny):
        outer[d] = go(remote(mine, mine, g_send.at[d], g_recv.at[d], away(d)), "wait_send")
    go(remote(mine, mine, h_send.at[0], h_recv.at[0], partner), "wait")
    in_grads(2, 4)
    for d in range(1, ny):
        outer[d].wait_recv()
        theirs = stream_ref.at[:, columns(lax.rem(y - d + ny, ny) * 2 + c)]
        go(remote(theirs, theirs, h_send.at[d], h_recv.at[d], partner), "wait")
    for wait in waits:
        wait()
    wide = blocks_ref.shape[2]
    for b in range(n):
        blocks_ref[b] = stream_ref[:, b * wide : (b + 1) * wide]


def main_part(n, ny, cap, ids, weights, decay, rows, grad, kept, gate_w, up_w, down_w):
    tokens, q = grad.shape
    dma = pltpu.SemaphoreType.DMA
    slots, model, width = n * cap, rows.shape[1], gate_w.shape[2]
    nz = n // 2
    vmem, anywhere = pl.BlockSpec(memory_space=pltpu.VMEM), pl.BlockSpec(memory_space=pl.ANY)
    return pl.pallas_call(
        functools.partial(main_kernel, n, ny, cap),
        out_shape=(
            jax.ShapeDtypeStruct((tokens, model), BF16),
            jax.ShapeDtypeStruct((n, tokens, model // n), BF16),
            jax.ShapeDtypeStruct((n,) + kept.shape, BF16),
            jax.ShapeDtypeStruct((n, 8, 128), F32),
            jax.ShapeDtypeStruct(gate_w.shape, BF16),
            jax.ShapeDtypeStruct(up_w.shape, BF16),
            jax.ShapeDtypeStruct(down_w.shape, BF16),
        ),
        in_specs=[vmem, vmem, vmem, anywhere, vmem, vmem, anywhere, anywhere, anywhere],
        out_specs=[vmem] * 7,
        scratch_shapes=[
            pltpu.VMEM((tokens, q), BF16),
            pltpu.VMEM(gate_w.shape[1:], BF16),
            pltpu.VMEM(up_w.shape[1:], BF16),
            pltpu.VMEM(down_w.shape[1:], BF16),
            pltpu.VMEM((slots, tokens), BF16),
            pltpu.VMEM((n, 2, cap, q), BF16),
            pltpu.VMEM((2, slots, model), BF16),
            pltpu.VMEM((slots, width), BF16),
            pltpu.VMEM((slots, 2 * width), BF16),
            pltpu.VMEM((slots, model), BF16),
            pltpu.VMEM((ny, slots, q), BF16),
            pltpu.VMEM((ny, slots, q), BF16),
            pltpu.VMEM((ny, slots, q), BF16),
            pltpu.VMEM((slots, q), BF16),
            pltpu.VMEM((slots, q), BF16),
            dma((4,)),
        ]
        + [dma((n,))] * 4
        + [dma((ny, n))] * 4
        + [dma((ny, nz))] * 4
        + [dma((n,))] * 2
        + [dma((ny,))] * 4
        + [dma((n,))] * 6,
        compiler_params=pltpu.CompilerParams(
            collective_id=0, has_side_effects=True, vmem_limit_bytes=LIMIT
        ),
    )(ids, weights, decay, rows, grad, kept, gate_w, up_w, down_w)


def tail_kernel(
    n, ny, stream_ref, state_ref, cols_ref, states_ref,
    local_sem, a_send, a_recv, i_send, i_recv, p_send, p_recv,
):
    s, t, y, c = where_am_i(n, ny)
    half = stream_ref.shape[1] // 2
    partner = (s, y * 2 + 1 - c)
    greet(sp_peers(n, s, t) + [partner])
    band = pl.ds(pl.multiple_of(c * half, half), half)
    own = [
        pltpu.make_async_copy(stream_ref.at[s], cols_ref.at[s], local_sem.at[0]),
        pltpu.make_async_copy(state_ref, states_ref.at[s], local_sem.at[1]),
    ]
    for copy in own:
        copy.start()
    waits, arrivals = [copy.wait for copy in own], []
    for k in range(1, n):
        peer = lax.rem(s + k, n)
        copy = remote(state_ref, states_ref.at[s], i_send.at[k], i_recv.at[k], (peer, t))
        copy.start()
        waits.append(copy.wait)
    for k in range(1, n):
        peer = lax.rem(s + k, n)
        copy = remote(
            stream_ref.at[peer, band], cols_ref.at[s, band], a_send.at[k], a_recv.at[k], (peer, t)
        )
        copy.start()
        waits.append(copy.wait_send)
        arrivals.append(copy)
    for k in range(1, n):
        arrivals[k - 1].wait_recv()
        held = cols_ref.at[lax.rem(s - k + n, n), band]
        copy = remote(held, held, p_send.at[k], p_recv.at[k], partner)
        copy.start()
        waits.append(copy.wait)
    for wait in waits:
        wait()


def tail_exchange(n, ny, stream, state):
    dma = pltpu.SemaphoreType.DMA
    return pl.pallas_call(
        functools.partial(tail_kernel, n, ny),
        out_shape=(
            jax.ShapeDtypeStruct(stream.shape, BF16),
            jax.ShapeDtypeStruct((n,) + state.shape, state.dtype),
        ),
        in_specs=[pl.BlockSpec(memory_space=pltpu.VMEM)] * 2,
        out_specs=[pl.BlockSpec(memory_space=pltpu.VMEM)] * 2,
        scratch_shapes=[dma((2,))] + [dma((n,))] * 6,
        compiler_params=pltpu.CompilerParams(
            collective_id=2, has_side_effects=True, vmem_limit_bytes=LIMIT
        ),
    )(stream, state)


def on_device(
    moe_input,
    out_grad,
    expert_ids,
    expert_weights,
    w_gate,
    w_up,
    w_down,
    out_proj,
    retained,
    queries,
    keys,
    values,
    log_decay,
    incoming_state,
):
    f32 = jnp.float32
    bf16 = jnp.bfloat16
    upper_limit = lax.Precision.HIGHEST
    tokens_here = moe_input.shape[0]
    sp_count = lax.axis_size("sp")
    tp_count = lax.axis_size("tp")
    capacity = -(-(5 * tokens_here // (2 * sp_count)) // 16) * 16
    along = (((0,), (0,)), ((), ()))
    ny = tp_count // 2
    heads_here = log_decay.shape[1]
    running_total = jnp.cumsum(log_decay, axis=0)
    last_sum = running_total[-1]
    stream, stream_blocks, kept_all, ends_all, gate_w_grad, up_w_grad, down_grad = main_part(
        sp_count, ny, capacity, expert_ids.T, expert_weights.T, log_decay.T, moe_input, out_grad,
        retained, w_gate, w_up, w_down,
    )
    ret_grad = lax.dot_general(
        stream, out_proj, (((1,), (1,)), ((), ())), preferred_element_type=f32
    ).astype(bf16)
    key_dim = queries.shape[1] // heads_here
    value_dim = values.shape[1] // heads_here
    query_rows = queries.astype(f32).reshape(tokens_here, heads_here, key_dim)
    key_matrix = keys.astype(f32).reshape(tokens_here, heads_here, key_dim)
    value_matrix = values.astype(f32).reshape(tokens_here, heads_here, value_dim)
    incoming_gradient = ret_grad.astype(f32).reshape(tokens_here, heads_here, value_dim)
    place = jnp.arange(tokens_here)
    causal = (place[:, None] >= place[None, :])[:, :, None]
    diff = running_total[:, None, :] - running_total[None, :, :]
    decay = jnp.where(causal, jnp.exp(jnp.minimum(diff, 0.0)), 0.0)
    scores = jnp.einsum("thk,shk->tsh", query_rows, key_matrix, precision=upper_limit) * decay
    prob_grad = (
        jnp.einsum("thv,shv->tsh", incoming_gradient, value_matrix, precision=upper_limit) * decay
    )
    added_input = jnp.einsum(
        "yb,ybm,ybx->bmx",
        jnp.exp(running_total),
        query_rows,
        incoming_gradient,
        precision=upper_limit,
    )
    flat_state = added_input.transpose(1, 0, 2).reshape(key_dim, heads_here * value_dim)
    stream_all, states = tail_exchange(sp_count, ny, stream_blocks, flat_state.astype(bf16))
    out_proj_grad = lax.dot_general(
        stream_all.reshape(sp_count * tokens_here, -1),
        kept_all.reshape(sp_count * tokens_here, -1),
        along,
        preferred_element_type=f32,
    )
    block_ends = ends_all[:, :heads_here, 0]
    before = jnp.cumsum(block_ends, axis=0) - block_ends
    here = lax.axis_index("sp")
    since = jnp.sum(
        jnp.where(jnp.arange(sp_count)[:, None] <= here, block_ends, 0.0), axis=0, keepdims=True
    )
    reach = jnp.where(
        jnp.arange(sp_count)[:, None] > here, jnp.exp(jnp.minimum(before - since, 0.0)), 0.0
    )
    state_gradient = jnp.sum(
        states.astype(f32).reshape(sp_count, key_dim, heads_here, value_dim)
        * reach[:, None, :, None],
        axis=0,
    ).transpose(1, 0, 2)
    tail = jnp.exp(last_sum[None, :] - running_total)[..., None]
    query_grad = jnp.einsum("tsh,shk->thk", prob_grad, key_matrix, precision=upper_limit) + jnp.exp(
        running_total
    )[..., None] * jnp.einsum(
        "ybc,bfc->ybf", incoming_gradient, incoming_state[0], precision=upper_limit
    )
    key_grad = jnp.einsum(
        "tsh,thk->shk", prob_grad, query_rows, precision=upper_limit
    ) + tail * jnp.einsum("rgd,gnd->rgn", value_matrix, state_gradient, precision=upper_limit)
    value_grad = jnp.einsum(
        "tsh,thv->shv", scores, incoming_gradient, precision=upper_limit
    ) + tail * jnp.einsum("bgi,gie->bge", key_matrix, state_gradient, precision=upper_limit)
    return (
        gate_w_grad,
        up_w_grad,
        down_grad,
        out_proj_grad,
        query_grad.reshape(tokens_here, -1).astype(bf16),
        key_grad.reshape(tokens_here, -1).astype(bf16),
        value_grad.reshape(tokens_here, -1).astype(bf16),
    )


def solution(mesh):
    placed = (
        P("sp", None),
        P("sp", "tp"),
        P("sp", None),
        P("sp", None),
        P("sp", None, "tp"),
        P("sp", None, "tp"),
        P("sp", "tp", None),
        P("tp", None),
        P("sp", "tp"),
        P("sp", "tp"),
        P("sp", "tp"),
        P("sp", "tp"),
        P("sp", "tp"),
        P("sp", "tp", None, None),
    )
    return jax.shard_map(
        on_device,
        mesh=mesh,
        in_specs=placed,
        out_specs=(
            P("sp", None, "tp"),
            P("sp", None, "tp"),
            P("sp", "tp", None),
            P("sp", "tp"),
            P("sp", "tp"),
            P("sp", "tp"),
            P("sp", "tp"),
        ),
        check_vma=False,
    )
```

```python
import functools

import jax
import jax.numpy as jnp
from jax import lax
from jax.experimental import pallas as pl
from jax.experimental.pallas import tpu as pltpu
from jax.sharding import PartitionSpec as P

MESH = pl.DeviceIdType.MESH
F32 = jnp.float32
BF16 = jnp.bfloat16
LIMIT = 38 * 1024 * 1024


def where_am_i(n, ny):
    s, t = lax.axis_index("sp"), lax.axis_index("tp")
    return s, t, lax.div(t, 2), lax.rem(t, 2)


def greet(peers):
    barrier = pltpu.get_barrier_semaphore()
    for peer in peers:
        pl.semaphore_signal(barrier, inc=1, device_id=peer, device_id_type=MESH)
    pl.semaphore_wait(barrier, len(peers))


def sp_peers(n, s, t):
    return [(lax.rem(s + k, n), t) for k in range(1, n)]


def tp_peers(ny, s, y, c):
    return [(s, lax.rem(y + d, ny) * 2 + c) for d in range(1, ny)] + [(s, y * 2 + 1 - c)]


def remote(src, dst, send, recv, peer):
    return pltpu.make_async_remote_copy(
        src_ref=src, dst_ref=dst, send_sem=send, recv_sem=recv, device_id=peer, device_id_type=MESH
    )


def below(a, b, top):
    return lax.div(b - a + top - 1, top)


def nearest_first(z, nz):
    high = nz - 1 - z
    fewer = below(high, z, nz)
    least = z + (high - z) * fewer
    toward = 1 - 2 * fewer
    order = [z]
    for i in range(1, nz):
        both = below(i, 2 * least + 1, 2 * nz)
        step = (i + 1) // 2 * (1 if i % 2 else -1)
        order.append(z + toward * (both * step + (1 - both) * (i - least)))
    return order


def main_kernel(
    n, ny, cap, ids_hbm, weights_hbm, decay_hbm, rows_hbm, grad_hbm, kept_hbm,
    gate_hbm, up_hbm, down_hbm, proj_hbm, query_hbm, key_hbm, value_hbm, incoming_hbm,
    kept_out, cols_ref, gate_grad_ref, up_grad_ref, down_grad_ref, query_out, key_out, value_out,
    stream_ref, ends_out, proj, incoming, o_ref, states, pair_state, reach, turn_out, turn_in,
    blocks, ids_ref, weights_ref, decay_ref, grad_ref, kept_ref, query_ref, key_ref, value_ref,
    incoming_ref, rows_v, gate_w, up_w, down_w, pick, send, slots, act, both_grads, part, near, pairs, far,
    share, back,
    load_sem, a_send, a_recv, e_send, e_recv, y_send, y_recv, p_send, p_recv,
    n_send, n_recv, f_send, f_recv, b_send, b_recv, g_send, g_recv, h_send, h_recv,
    r_send, r_recv, l_send, l_recv, x_send, x_recv,
    s_send, s_recv, u_send, u_recv, c_send, c_recv, v_send, v_recv, w_send, w_recv,
):
    s, t, y, c = where_am_i(n, ny)
    tokens, q = grad_ref.shape
    heads = decay_ref.shape[0]
    width = gate_w.shape[1]
    nz = n // 2
    z, x = lax.div(s, 2), lax.rem(s, 2)
    partner = (s, y * 2 + 1 - c)
    order = nearest_first(z, nz)
    waits = []

    def columns(tt):
        return pl.ds(pl.multiple_of(tt * q, q), q)

    def block_rows(b):
        return pl.ds(pl.multiple_of(b * cap, cap), cap)

    def chunk_rows(i):
        return pl.ds(pl.multiple_of(order[i] * 2 * cap, 2 * cap), 2 * cap)

    def member(i, e):
        return order[i] * 2 + (x if e == 0 else 1 - x)

    def away(d):
        return (s, lax.rem(y + d, ny) * 2 + c)

    def go(copy, wait):
        copy.start()
        waits.append(getattr(copy, wait))
        return copy

    barrier = pltpu.get_barrier_semaphore()
    peers = sp_peers(n, s, t) + tp_peers(ny, s, y, c)
    for peer in peers:
        pl.semaphore_signal(barrier, inc=1, device_id=peer, device_id_type=MESH)

    loads = [
        pltpu.make_async_copy(hbm, local, load_sem.at[j])
        for j, (hbm, local) in enumerate(
            [
                (ids_hbm, ids_ref), (weights_hbm, weights_ref), (decay_hbm, decay_ref),
                (grad_hbm, grad_ref), (rows_hbm.at[:, columns(t)], rows_v), (kept_hbm, kept_ref),
                (gate_hbm.at[0], gate_w), (up_hbm.at[0], up_w), (down_hbm.at[0], down_w),
                (proj_hbm, proj), (query_hbm, query_ref), (key_hbm, key_ref),
                (value_hbm, value_ref), (incoming_hbm, incoming_ref),
            ]
        )
    ]
    for copy in loads:
        copy.start()
    for copy in loads[:6]:
        copy.wait()

    ids = ids_ref[...].astype(F32)
    ids = [ids[j : j + 1, :] for j in range(2)]
    weights = [weights_ref[j : j + 1, :] for j in range(2)]
    expert_row = lax.broadcasted_iota(jnp.int32, (n, tokens), 0).astype(F32)
    named = [(expert_row == own).astype(F32) for own in ids]
    first = lax.broadcasted_iota(jnp.int32, (tokens, tokens), 0)
    second = lax.broadcasted_iota(jnp.int32, (tokens, tokens), 1)
    earlier = jnp.dot(
        (named[0] + named[1]).astype(BF16),
        (first < second).astype(F32).astype(BF16),
        preferred_element_type=F32,
    )
    slot = [
        own * cap + jnp.sum(hot * earlier, axis=0, keepdims=True) for own, hot in zip(ids, named)
    ]
    number = lax.broadcasted_iota(jnp.int32, (n * cap, tokens), 0).astype(F32)
    hits = [(number == own).astype(F32) for own in slot]
    picker = (hits[0] + hits[1]).astype(BF16)
    slot_weight = jnp.sum(hits[0] * weights[0] + hits[1] * weights[1], axis=1, keepdims=True)
    pick[...] = picker
    ends_out[s, :, :] = jnp.zeros((8, 128), F32)
    ends_out[s, pl.ds(0, heads), :] = jnp.broadcast_to(
        jnp.sum(decay_ref[...], axis=1, keepdims=True), (heads, 128)
    )
    cotangent = jnp.dot(picker, grad_ref[...], preferred_element_type=F32) * slot_weight
    send[:, 1] = cotangent.astype(BF16).reshape(n, cap, q)
    picked = jnp.dot(picker, rows_v[...], preferred_element_type=F32).astype(BF16)
    send[:, 0] = picked.reshape(n, cap, q)
    slots[0, block_rows(s), columns(t)] = send[s, 0]
    slots[1, block_rows(s), columns(t)] = send[s, 1]

    pl.semaphore_wait(barrier, len(peers))

    def block(src, tt):
        return slots.at[:, block_rows(src), columns(tt)]

    for i in range(nz):
        for e in range(2):
            if (i, e) != (0, 0):
                to = member(i, e)
                go(
                    remote(send.at[to], block(s, t), a_send.at[2 * i + e], a_recv.at[s], (to, t)),
                    "wait_send",
                )

    def at(zz):
        return lax.rem(zz + 2 * nz, nz) * 2 + x

    def hop(j, sign, send_sem, recv_sem, source):
        held = at(z - sign * j)
        return go(
            remote(
                source, kept_out.at[held], send_sem.at[j], recv_sem.at[j], (at(z + sign), t)
            ),
            "wait_send",
        )

    def across(held, index, source):
        go(
            remote(
                source, kept_out.at[held], x_send.at[index], x_recv.at[index],
                (z * 2 + 1 - x, t),
            ),
            "wait",
        )

    right_steps, left_steps = nz // 2, nz - 1 - nz // 2
    moving = {}

    def kept_start():
        if right_steps:
            moving["right"] = hop(0, 1, r_send, r_recv, kept_ref)
        if left_steps:
            moving["left"] = hop(0, -1, l_send, l_recv, kept_ref)
        across(s, 0, kept_ref)
        kept_out[s] = kept_ref[...]

    def kept_relay(j):
        if j <= right_steps:
            moving["right"].wait_recv()
            held = at(z - j)
            if j < right_steps:
                moving["right"] = hop(j, 1, r_send, r_recv, kept_out.at[held])
            across(held, 2 * j - 1, kept_out.at[held])
        if j <= left_steps:
            moving["left"].wait_recv()
            held = at(z + j)
            if j < left_steps:
                moving["left"] = hop(j, -1, l_send, l_recv, kept_out.at[held])
            across(held, 2 * j, kept_out.at[held])

    from_far, from_partner = {}, {}

    def arrive(i, e):
        src = member(i, e)
        mine = block(src, t)
        if (i, e) != (0, 0):
            remote(
                send.at[src], mine, a_send.at[2 * i + e], a_recv.at[src], (src, t)
            ).wait_recv()
        k = 2 * i + e
        for d in range(1, ny):
            from_far[d, k] = go(
                remote(mine, mine, y_send.at[d, k], y_recv.at[d, k], away(d)), "wait_send"
            )
        from_partner[0, k] = go(
            remote(mine, mine, p_send.at[0, k], p_recv.at[0, k], partner), "wait_send"
        )

    def relay(i, e):
        k = 2 * i + e
        for d in range(1, ny):
            from_far[d, k].wait_recv()
            theirs = block(member(i, e), lax.rem(y - d + ny, ny) * 2 + c)
            from_partner[d, k] = go(
                remote(theirs, theirs, p_send.at[d, k], p_recv.at[d, k], partner), "wait_send"
            )

    across_dims = (((1,), (1,)), ((), ()))
    along_dims = (((0,), (0,)), ((), ()))

    def expert(i):
        for e in range(2):
            for d in range(ny):
                from_partner[d, 2 * i + e].wait_recv()
        r = chunk_rows(i)
        gate = jnp.dot(slots[0, r, :], gate_w[...], preferred_element_type=F32)
        up = jnp.dot(slots[0, r, :], up_w[...], preferred_element_type=F32)
        act_grad = lax.dot_general(
            slots[1, r, :], down_w[...], across_dims, preferred_element_type=F32
        )
        sig = jax.nn.sigmoid(gate)
        swish = gate * sig
        act[r, :] = (swish * up).astype(BF16)
        gate_grad = (act_grad * up * sig * (1.0 + gate * (1.0 - sig))).astype(BF16)
        up_grad = (act_grad * swish).astype(BF16)
        both_grads[r, pl.ds(0, width)] = gate_grad
        both_grads[r, pl.ds(width, width)] = up_grad
        part[r, :] = (
            lax.dot_general(gate_grad, gate_w[...], across_dims, preferred_element_type=F32)
            + lax.dot_general(up_grad, up_w[...], across_dims, preferred_element_type=F32)
        ).astype(BF16)

    halves, summed, returns = {}, {}, {}

    def swap_halves(i):
        r = chunk_rows(i)
        for d in list(range(1, ny)) + [0]:
            theirs = lax.rem(y + d, ny) * 2 + 1 - c
            halves[d, i] = go(
                remote(
                    part.at[r, columns(theirs)], near.at[d, r, :],
                    n_send.at[d, i], n_recv.at[d, i], partner,
                ),
                "wait_send",
            )

    def send_pairs(i):
        r = chunk_rows(i)
        for d in range(1, ny):
            halves[d, i].wait_recv()
            tt = lax.rem(y + d, ny) * 2 + c
            pairs[d, r, :] = (
                part[r, columns(tt)].astype(F32) + near[d, r, :].astype(F32)
            ).astype(BF16)
            summed[d, i] = go(
                remote(
                    pairs.at[d, r, :], far.at[d, r, :], f_send.at[d, i], f_recv.at[d, i], (s, tt)
                ),
                "wait_send",
            )

    def send_back(i):
        r = chunk_rows(i)
        halves[0, i].wait_recv()
        total = part[r, columns(t)].astype(F32) + near[0, r, :].astype(F32)
        for d in range(1, ny):
            summed[d, i].wait_recv()
            total = total + far[d, r, :].astype(F32)
        share[r, :] = total.astype(BF16)
        for e in range(2):
            to = member(i, e)
            if (i, e) == (0, 0):
                back[block_rows(s), :] = share[block_rows(s), :]
            else:
                go(
                    remote(
                        share.at[block_rows(to), :], back.at[block_rows(s), :],
                        b_send.at[2 * i + e], b_recv.at[s], (to, t),
                    ),
                    "wait_send",
                )

    def returned(i):
        for e in range(2):
            if (i, e) != (0, 0):
                src = member(i, e)
                remote(
                    share.at[block_rows(src), :], back.at[block_rows(src), :],
                    b_send.at[2 * i + e], b_recv.at[src], (src, t),
                ).wait_recv()
        r = chunk_rows(i)
        return lax.dot_general(
            pick[r, :], back[r, :], along_dims, preferred_element_type=F32
        )

    def down_grads():
        turned = act[...].T
        wide = 512
        for j in range(0, down_grad_ref.shape[2], wide):
            down_grad_ref[0, :, j : j + wide] = jnp.dot(
                turned, slots[1, :, j : j + wide], preferred_element_type=F32
            ).astype(BF16)

    def in_grads(lo, hi):
        tall = 256

        def step(j, carry):
            band = pl.ds(pl.multiple_of(j * tall, tall), tall)
            grads = lax.dot_general(
                slots[0, :, band], both_grads[...], along_dims, preferred_element_type=F32
            ).astype(BF16)
            gate_grad_ref[0, band, :] = grads[:, :width]
            up_grad_ref[0, band, :] = grads[:, width:]
            return carry

        count = gate_grad_ref.shape[1] // tall
        lax.fori_loop(lo * count // 4, hi * count // 4, step, 0)

    ends_moving = []
    for k in range(1, n):
        to = lax.rem(s + k, n)
        ends_moving.append(
            go(
                remote(ends_out.at[s], ends_out.at[s], e_send.at[k], e_recv.at[k], (to, t)),
                "wait_send",
            )
        )
    kept_start()
    for i in range(nz + 1):
        if i < nz:
            arrive(i, 0)
            arrive(i, 1)
        if i == 1:
            for copy in loads[6:]:
                copy.wait()
        if i >= 1:
            relay(i - 1, 0)
            relay(i - 1, 1)
        if i >= 2:
            send_pairs(i - 2)
        if i >= 3:
            send_back(i - 3)
        if i >= 1:
            expert(i - 1)
            swap_halves(i - 1)
        if i >= 2:
            kept_relay(i - 1)
    send_back(nz - 2) if nz > 1 else None
    send_pairs(nz - 1)
    down_grads()
    send_back(nz - 1)
    in_grads(0, 2)
    token = returned(0)
    for i in range(1, nz):
        token = token + returned(i)
    stream_ref[:, columns(t)] = (grad_ref[...].astype(F32) + token).astype(BF16)
    mine = stream_ref.at[:, columns(t)]
    outer = {}
    for d in range(1, ny):
        outer[d] = go(remote(mine, mine, g_send.at[d], g_recv.at[d], away(d)), "wait_send")
    inner = {}
    inner[0] = go(remote(mine, mine, h_send.at[0], h_recv.at[0], partner), "wait_send")
    in_grads(2, 4)
    for d in range(1, ny):
        outer[d].wait_recv()
        theirs = stream_ref.at[:, columns(lax.rem(y - d + ny, ny) * 2 + c)]
        inner[d] = go(
            remote(theirs, theirs, h_send.at[d], h_recv.at[d], partner), "wait_send"
        )
    band_count = 2 * ny if tokens % (32 * ny) == 0 else 2
    tall = tokens // band_count
    wide = cols_ref.shape[2]
    tp_bands = band_count > 2

    def band(yy, cc):
        return pl.ds(pl.multiple_of((yy * 2 + cc if tp_bands else cc) * tall, tall), tall)

    value_dim, key_dim = value_ref.shape[1] // heads, key_ref.shape[1] // heads
    ret = lax.dot_general(
        stream_ref[:, columns(t)], proj[:, columns(t)], across_dims, preferred_element_type=F32
    )
    for d in range(1, ny):
        tt = lax.rem(y - d + ny, ny) * 2 + c
        ret = ret + lax.dot_general(
            stream_ref[:, columns(tt)], proj[:, columns(tt)], across_dims,
            preferred_element_type=F32,
        )
    for d in range(ny):
        inner[d].wait_recv()
        tt = lax.rem(y - d + ny, ny) * 2 + 1 - c
        ret = ret + lax.dot_general(
            stream_ref[:, columns(tt)], proj[:, columns(tt)], across_dims,
            preferred_element_type=F32,
        )
    o_ref[...] = ret.astype(BF16)

    def expand(rows, width, depth):
        lane = lax.div(lax.broadcasted_iota(jnp.int32, (rows[0].shape[0], width), 1), depth)
        out = jnp.zeros((rows[0].shape[0], width), F32)
        for h in range(heads):
            out = jnp.where(lane == h, jnp.broadcast_to(rows[h], out.shape), out)
        return out

    key_width, value_width = heads * key_dim, heads * value_dim
    exact = lax.Precision.HIGHEST
    low = (first >= second).astype(F32)
    total = lax.dot_general(
        low, decay_ref[...], across_dims, precision=exact, preferred_element_type=F32
    )
    total_row = lax.dot_general(
        decay_ref[...], low, across_dims, precision=exact, preferred_element_type=F32
    )
    head_total = [total[:, h : h + 1] for h in range(heads)]
    head_row = [total_row[h : h + 1, :] for h in range(heads)]
    head_end = [total[tokens - 1 : tokens, h : h + 1] for h in range(heads)]
    grown = jnp.exp(expand(head_total, key_width, key_dim))
    state_row = lax.div(lax.broadcasted_iota(jnp.int32, (key_width, value_width), 0), key_dim)
    state_lane = lax.div(lax.broadcasted_iota(jnp.int32, (key_width, value_width), 1), value_dim)
    diagonal = state_row == state_lane
    injected = lax.dot_general(
        (query_ref[...].astype(F32) * grown).astype(BF16), o_ref[...], along_dims,
        preferred_element_type=F32,
    )
    injected = jnp.where(diagonal, injected, 0.0)
    folded = injected[:key_dim, :]
    for h in range(1, heads):
        folded = folded + injected[h * key_dim : (h + 1) * key_dim, :]
    states[z] = folded.astype(BF16)
    pair_copy = go(
        remote(states.at[z], pair_state, u_send.at[0], u_recv.at[0], (z * 2 + 1 - x, t)),
        "wait_send",
    )
    for i in range(1, nz):
        go(
            remote(
                states.at[z], states.at[z], s_send.at[i], s_recv.at[z], (order[i] * 2 + x, t)
            ),
            "wait_send",
        )

    def piece(b, rows):
        if wide % 128:
            return blocks.at[b, rows]
        return stream_ref.at[rows, pl.ds(pl.multiple_of(b * wide, wide), wide)]

    if wide % 128:
        for b in range(n):
            blocks[b] = stream_ref[:, b * wide : (b + 1) * wide]

    for i in range(nz):
        for e in range(2):
            if (i, e) != (0, 0):
                to = member(i, e)
                go(
                    remote(
                        piece(to, band(y, c)), cols_ref.at[s, band(y, c)],
                        c_send.at[2 * i + e], c_recv.at[s], (to, t),
                    ),
                    "wait_send",
                )
    cols_ref[s] = piece(s, pl.ds(0, tokens))[...]

    for copy in ends_moving:
        copy.wait_recv()
    before = [jnp.zeros((1, value_width), F32)]
    since = jnp.zeros((1, value_width), F32)
    for b in range(n):
        ends = expand([ends_out[b, h : h + 1, 0:1] for h in range(heads)], value_width, value_dim)
        before.append(before[-1] + ends)
        since = since + ends * below(b, 2 * z + 2, 2 * n).astype(F32)
    for b in range(n):
        reach[b] = jnp.broadcast_to(
            jnp.exp(jnp.minimum(before[b] - since, 0.0)) * below(2 * z + 1, b, 2 * n).astype(F32),
            (8, value_width),
        )

    key_lane = lax.div(lax.broadcasted_iota(jnp.int32, (tokens, key_width), 1), key_dim)
    value_lane = lax.div(lax.broadcasted_iota(jnp.int32, (tokens, value_width), 1), value_dim)

    def only(values, lane, h):
        return jnp.where(lane == h, values, jnp.zeros_like(values))

    place = lax.broadcasted_iota(jnp.int32, (value_dim, value_width), 0)
    spot = lax.broadcasted_iota(jnp.int32, (value_dim, value_width), 1)
    for h in range(heads):
        put = (place + h * value_dim == spot).astype(F32).astype(BF16)
        incoming[h * key_dim : (h + 1) * key_dim, :] = jnp.dot(
            incoming_ref[0, h].astype(BF16), put, preferred_element_type=F32
        ).astype(BF16)
    query_grad = grown * lax.dot_general(
        o_ref[...], incoming[...], across_dims, preferred_element_type=F32
    )
    key_grad = jnp.zeros((tokens, key_width), F32)
    value_grad = jnp.zeros((tokens, value_width), F32)
    for h in range(heads):
        o_head = only(o_ref[...], value_lane, h)
        v_head = only(value_ref[...], value_lane, h)
        q_head = only(query_ref[...], key_lane, h)
        k_head = only(key_ref[...], key_lane, h)
        diff = head_total[h] - head_row[h]
        fade = jnp.where(first >= second, jnp.exp(jnp.minimum(diff, 0.0)), 0.0)
        fade_turned = jnp.where(first <= second, jnp.exp(jnp.minimum(-diff, 0.0)), 0.0)
        prob = lax.dot_general(o_head, value_ref[...], across_dims, preferred_element_type=F32)
        query_grad = query_grad + jnp.dot(
            (prob * fade).astype(BF16), k_head, preferred_element_type=F32
        )
        prob = lax.dot_general(v_head, o_ref[...], across_dims, preferred_element_type=F32)
        key_grad = key_grad + jnp.dot(
            (prob * fade_turned).astype(BF16), q_head, preferred_element_type=F32
        )
        score = lax.dot_general(k_head, query_ref[...], across_dims, preferred_element_type=F32)
        value_grad = value_grad + jnp.dot(
            (score * fade_turned).astype(BF16), o_head, preferred_element_type=F32
        )
    query_out[...] = query_grad.astype(BF16)

    later = jnp.zeros((key_dim, value_width), F32)
    for i in range(1, nz):
        src = order[i]
        remote(
            states.at[src], states.at[src], s_send.at[i], s_recv.at[src], (src * 2 + x, t)
        ).wait_recv()
        later = later + reach[src * 2 + x][0:1, :] * states[src].astype(F32)
    turn_out[...] = later.astype(BF16)
    turned = go(
        remote(turn_out, turn_in, u_send.at[1], u_recv.at[1], (z * 2 + 1 - x, t)), "wait_send"
    )

    from_far, from_partner = {}, {}
    for i in range(nz):
        for e in range(2):
            if (i, e) == (0, 0):
                continue
            src, k = member(i, e), 2 * i + e
            mine = cols_ref.at[src, band(y, c)]
            remote(
                piece(src, band(y, c)), mine, c_send.at[k], c_recv.at[src],
                (src, t),
            ).wait_recv()
            if tp_bands:
                for d in range(1, ny):
                    from_far[d, k] = go(
                        remote(mine, mine, v_send.at[d, k], v_recv.at[d, k], away(d)),
                        "wait_send",
                    )
            go(remote(mine, mine, w_send.at[0, k], w_recv.at[0, k], partner), "wait")
    turned.wait_recv()
    later = turn_out[...].astype(F32) + turn_in[...].astype(F32)
    lower = (1 - x).astype(F32)
    pair_ends = expand(
        [ends_out[z * 2 + 1, h : h + 1, 0:1] for h in range(heads)], value_width, value_dim
    )
    pair_copy.wait_recv()
    later = jnp.exp(lower * pair_ends) * later + lower * pair_state[...].astype(F32)
    stacked = jnp.concatenate([later.astype(BF16)] * heads, axis=0)
    stacked = jnp.where(diagonal, stacked, jnp.zeros_like(stacked))
    left = [end - own for end, own in zip(head_end, head_total)]
    key_grad = key_grad + jnp.exp(expand(left, key_width, key_dim)) * lax.dot_general(
        value_ref[...], stacked, across_dims, preferred_element_type=F32
    )
    key_out[...] = key_grad.astype(BF16)
    value_grad = value_grad + jnp.exp(expand(left, value_width, value_dim)) * jnp.dot(
        key_ref[...], stacked, preferred_element_type=F32
    )
    value_out[...] = value_grad.astype(BF16)
    if tp_bands:
        for i in range(nz):
            for e in range(2):
                if (i, e) == (0, 0):
                    continue
                src, k = member(i, e), 2 * i + e
                for d in range(1, ny):
                    from_far[d, k].wait_recv()
                    theirs = cols_ref.at[src, band(lax.rem(y - d + ny, ny), c)]
                    go(
                        remote(theirs, theirs, w_send.at[d, k], w_recv.at[d, k], partner), "wait"
                    )
    for wait in waits:
        wait()


def main_part(
    n, ny, cap, ids, weights, decay, rows, grad, kept, gate_w, up_w, down_w, proj, query, key,
    value, incoming,
):
    tokens, q = grad.shape
    heads = decay.shape[0]
    dma = pltpu.SemaphoreType.DMA
    slots, model, width = n * cap, rows.shape[1], gate_w.shape[2]
    nz = n // 2
    state = (key.shape[1] // heads, value.shape[1])
    vmem = pl.BlockSpec(memory_space=pltpu.VMEM)
    return pl.pallas_call(
        functools.partial(main_kernel, n, ny, cap),
        out_shape=(
            jax.ShapeDtypeStruct((n,) + kept.shape, BF16),
            jax.ShapeDtypeStruct((n, tokens, model // n), BF16),
            jax.ShapeDtypeStruct(gate_w.shape, BF16),
            jax.ShapeDtypeStruct(up_w.shape, BF16),
            jax.ShapeDtypeStruct(down_w.shape, BF16),
            jax.ShapeDtypeStruct(query.shape, BF16),
            jax.ShapeDtypeStruct(key.shape, BF16),
            jax.ShapeDtypeStruct(value.shape, BF16),
        ),
        in_specs=[pl.BlockSpec(memory_space=pltpu.HBM)] * 14,
        out_specs=[vmem] * 8,
        scratch_shapes=[
            pltpu.VMEM((tokens, model), BF16),
            pltpu.VMEM((n, 8, 128), F32),
            pltpu.VMEM(proj.shape, BF16),
            pltpu.VMEM((key.shape[1], value.shape[1]), BF16),
            pltpu.VMEM((tokens, value.shape[1]), BF16),
            pltpu.VMEM((nz,) + state, BF16),
            pltpu.VMEM(state, BF16),
            pltpu.VMEM((n, 8, value.shape[1]), F32),
            pltpu.VMEM(state, BF16),
            pltpu.VMEM(state, BF16),
            pltpu.VMEM((n, tokens, model // n) if model // n % 128 else (1, 8, 128), BF16),
            pltpu.VMEM(ids.shape, jnp.int32),
            pltpu.VMEM(weights.shape, F32),
            pltpu.VMEM(decay.shape, F32),
            pltpu.VMEM(grad.shape, BF16),
            pltpu.VMEM(kept.shape, BF16),
            pltpu.VMEM(query.shape, BF16),
            pltpu.VMEM(key.shape, BF16),
            pltpu.VMEM(value.shape, BF16),
            pltpu.VMEM(incoming.shape, F32),
            pltpu.VMEM((tokens, q), BF16),
            pltpu.VMEM(gate_w.shape[1:], BF16),
            pltpu.VMEM(up_w.shape[1:], BF16),
            pltpu.VMEM(down_w.shape[1:], BF16),
            pltpu.VMEM((slots, tokens), BF16),
            pltpu.VMEM((n, 2, cap, q), BF16),
            pltpu.VMEM((2, slots, model), BF16),
            pltpu.VMEM((slots, width), BF16),
            pltpu.VMEM((slots, 2 * width), BF16),
            pltpu.VMEM((slots, model), BF16),
            pltpu.VMEM((ny, slots, q), BF16),
            pltpu.VMEM((ny, slots, q), BF16),
            pltpu.VMEM((ny, slots, q), BF16),
            pltpu.VMEM((slots, q), BF16),
            pltpu.VMEM((slots, q), BF16),
            dma((14,)),
        ]
        + [dma((n,))] * 4
        + [dma((ny, n))] * 4
        + [dma((ny, nz))] * 4
        + [dma((n,))] * 2
        + [dma((ny,))] * 4
        + [dma((n,))] * 6
        + [dma((nz,))] * 2
        + [dma((2,))] * 2
        + [dma((n,))] * 2
        + [dma((ny, n))] * 4,
        compiler_params=pltpu.CompilerParams(
            collective_id=0, has_side_effects=True, vmem_limit_bytes=LIMIT
        ),
    )(
        *(
            pltpu.with_memory_space_constraint(array, pltpu.HBM)
            for array in (
                ids, weights, decay, rows, grad, kept, gate_w, up_w, down_w, proj, query, key,
                value, incoming,
            )
        )
    )


def final_kernel(cols_ref, kept_ref, *refs):
    moved = len(refs) // 2
    sources, proj_grad, targets, sems = (
        refs[:moved - 1], refs[moved - 1], refs[moved:-1], refs[-1]
    )
    copies = [
        pltpu.make_async_copy(source, target, sems.at[j])
        for j, (source, target) in enumerate(zip(sources, targets))
    ]
    for copy in copies:
        copy.start()
    rows = cols_ref.shape[0] * cols_ref.shape[1]
    proj_grad[...] = lax.dot_general(
        cols_ref[...].reshape(rows, -1), kept_ref[...].reshape(rows, -1),
        (((0,), (0,)), ((), ())), preferred_element_type=F32,
    )
    for copy in copies:
        copy.wait()


def final_part(cols, kept, *moved):
    vmem = pl.BlockSpec(memory_space=pltpu.VMEM)
    return pl.pallas_call(
        final_kernel,
        out_shape=(jax.ShapeDtypeStruct((cols.shape[2], kept.shape[2]), F32),)
        + tuple(jax.ShapeDtypeStruct(array.shape, array.dtype) for array in moved),
        in_specs=[vmem] * (2 + len(moved)),
        out_specs=[vmem] + [pl.BlockSpec(memory_space=pltpu.HBM)] * len(moved),
        scratch_shapes=[pltpu.SemaphoreType.DMA((len(moved),))],
        compiler_params=pltpu.CompilerParams(vmem_limit_bytes=LIMIT // 4),
    )(cols, kept, *moved)


def on_device(
    moe_input,
    out_grad,
    expert_ids,
    expert_weights,
    w_gate,
    w_up,
    w_down,
    out_proj,
    retained,
    queries,
    keys,
    values,
    log_decay,
    incoming_state,
):
    n, ny = lax.axis_size("sp"), lax.axis_size("tp") // 2
    tokens_here = moe_input.shape[0]
    capacity = -(-(5 * tokens_here // (2 * n)) // 16) * 16
    kept_all, cols, *moved = main_part(
        n, ny, capacity, expert_ids.T, expert_weights.T, log_decay.T, moe_input, out_grad,
        retained, w_gate, w_up, w_down, out_proj, queries, keys, values, incoming_state,
    )
    proj_grad, gate_grad, up_grad, down_grad, query_grad, key_grad, value_grad = final_part(
        cols, kept_all, *moved
    )
    return gate_grad, up_grad, down_grad, proj_grad, query_grad, key_grad, value_grad


def solution(mesh):
    placed = (
        P("sp", None),
        P("sp", "tp"),
        P("sp", None),
        P("sp", None),
        P("sp", None, "tp"),
        P("sp", None, "tp"),
        P("sp", "tp", None),
        P("tp", None),
        P("sp", "tp"),
        P("sp", "tp"),
        P("sp", "tp"),
        P("sp", "tp"),
        P("sp", "tp"),
        P("sp", "tp", None, None),
    )
    return jax.shard_map(
        on_device,
        mesh=mesh,
        in_specs=placed,
        out_specs=(
            P("sp", None, "tp"),
            P("sp", None, "tp"),
            P("sp", "tp", None),
            P("sp", "tp"),
            P("sp", "tp"),
            P("sp", "tp"),
            P("sp", "tp"),
        ),
        check_vma=False,
    )
```

```python
import functools

import jax
import jax.numpy as jnp
from jax import lax
from jax.experimental import pallas as pl
from jax.experimental.pallas import tpu as pltpu
from jax.sharding import PartitionSpec as P

MESH = pl.DeviceIdType.MESH
F32 = jnp.float32
BF16 = jnp.bfloat16
LIMIT = 38 * 1024 * 1024
AHEAD = 5


def where_am_i(n, ny):
    s, t = lax.axis_index("sp"), lax.axis_index("tp")
    return s, t, lax.div(t, 2), lax.rem(t, 2)


def greet(peers):
    barrier = pltpu.get_barrier_semaphore()
    for peer in peers:
        pl.semaphore_signal(barrier, inc=1, device_id=peer, device_id_type=MESH)
    pl.semaphore_wait(barrier, len(peers))


def sp_peers(n, s, t):
    return [(lax.rem(s + k, n), t) for k in range(1, n)]


def tp_peers(ny, s, y, c):
    return [(s, lax.rem(y + d, ny) * 2 + c) for d in range(1, ny)] + [(s, y * 2 + 1 - c)]


def remote(src, dst, send, recv, peer):
    return pltpu.make_async_remote_copy(
        src_ref=src, dst_ref=dst, send_sem=send, recv_sem=recv, device_id=peer, device_id_type=MESH
    )


def below(a, b, top):
    return lax.div(b - a + top - 1, top)


def flipped(z, i, nz):
    if nz & (nz - 1):
        return lax.rem(z + i, nz)
    out, bit = 0, 1
    while bit < nz:
        own = lax.rem(lax.div(z, bit), 2)
        out = out + bit * (1 - own if i & bit else own)
        bit *= 2
    return out


def main_kernel(
    n, ny, cap, ids_hbm, weights_hbm, decay_hbm, rows_hbm, grad_hbm, kept_hbm,
    gate_hbm, up_hbm, down_hbm, proj_hbm, query_hbm, key_hbm, value_hbm, incoming_hbm,
    proj_grad, gate_grad_ref, up_grad_ref, down_grad_ref, query_out, key_out, value_out,
    kept_out, cols_ref, stream_ref, ends_out, proj, incoming, o_ref, states, own_state, pair_state, reach, both_halves,
    later_halves,
    blocks, fade, fade_turned, score, ids_ref, weights_ref, decay_ref, grad_ref, kept_ref, query_ref, key_ref, value_ref,
    incoming_ref, rows_v, gate_w, up_w, down_w, pick, send, slots, act, both_grads, part, near, pairs, far,
    share, back,
    load_sem, a_send, a_recv, e_send, e_recv, y_send, y_recv, p_send, p_recv,
    n_send, n_recv, f_send, f_recv, b_send, b_recv, g_send, g_recv, h_send, h_recv,
    r_send, r_recv, l_send, l_recv, x_send, x_recv,
    s_send, s_recv, u_send, u_recv, c_send, c_recv, v_send, v_recv, w_send, w_recv,
):
    s, t, y, c = where_am_i(n, ny)
    tokens, q = grad_ref.shape
    heads = decay_ref.shape[0]
    width = gate_w.shape[1]
    nz = n // 2
    z, x = lax.div(s, 2), lax.rem(s, 2)
    partner = (s, y * 2 + 1 - c)
    order = [flipped(z, i, nz) for i in range(nz)]
    waits = []

    def columns(tt):
        return pl.ds(pl.multiple_of(tt * q, q), q)

    def block_rows(b):
        return pl.ds(pl.multiple_of(b * cap, cap), cap)

    def chunk_rows(i):
        return pl.ds(pl.multiple_of(order[i] * 2 * cap, 2 * cap), 2 * cap)

    def member(i, e):
        return order[i] * 2 + (x if e == 0 else 1 - x)

    def away(d):
        return (s, lax.rem(y + d, ny) * 2 + c)

    def go(copy, wait):
        copy.start()
        waits.append(getattr(copy, wait))
        return copy

    barrier = pltpu.get_barrier_semaphore()
    peers = sp_peers(n, s, t) + tp_peers(ny, s, y, c)
    for peer in peers:
        pl.semaphore_signal(barrier, inc=1, device_id=peer, device_id_type=MESH)

    loads = [
        pltpu.make_async_copy(hbm, local, load_sem.at[j])
        for j, (hbm, local) in enumerate(
            [
                (ids_hbm, ids_ref), (weights_hbm, weights_ref), (decay_hbm, decay_ref),
                (grad_hbm, grad_ref), (rows_hbm.at[:, columns(t)], rows_v), (kept_hbm, kept_ref),
                (gate_hbm.at[0], gate_w), (up_hbm.at[0], up_w), (down_hbm.at[0], down_w),
                (proj_hbm, proj), (query_hbm, query_ref), (key_hbm, key_ref),
                (value_hbm, value_ref), (incoming_hbm, incoming_ref),
            ]
        )
    ]
    for copy in loads:
        copy.start()
    for copy in loads[:6]:
        copy.wait()

    ids = ids_ref[...].astype(F32)
    ids = [ids[j : j + 1, :] for j in range(2)]
    weights = [weights_ref[j : j + 1, :] for j in range(2)]
    expert_row = lax.broadcasted_iota(jnp.int32, (n, tokens), 0).astype(F32)
    named = [(expert_row == own).astype(F32) for own in ids]
    first = lax.broadcasted_iota(jnp.int32, (tokens, tokens), 0)
    second = lax.broadcasted_iota(jnp.int32, (tokens, tokens), 1)
    earlier = jnp.dot(
        (named[0] + named[1]).astype(BF16),
        (first < second).astype(F32).astype(BF16),
        preferred_element_type=F32,
    )
    slot = [
        own * cap + jnp.sum(hot * earlier, axis=0, keepdims=True) for own, hot in zip(ids, named)
    ]
    number = lax.broadcasted_iota(jnp.int32, (n * cap, tokens), 0).astype(F32)
    hits = [(number == own).astype(F32) for own in slot]
    picker = (hits[0] + hits[1]).astype(BF16)
    slot_weight = jnp.sum(hits[0] * weights[0] + hits[1] * weights[1], axis=1, keepdims=True)
    pick[...] = picker
    ends_out[s, :, :] = jnp.zeros((8, 128), F32)
    ends_out[s, pl.ds(0, heads), :] = jnp.broadcast_to(
        jnp.sum(decay_ref[...], axis=1, keepdims=True), (heads, 128)
    )
    cotangent = jnp.dot(picker, grad_ref[...], preferred_element_type=F32) * slot_weight
    send[:, 1] = cotangent.astype(BF16).reshape(n, cap, q)
    picked = jnp.dot(picker, rows_v[...], preferred_element_type=F32).astype(BF16)
    send[:, 0] = picked.reshape(n, cap, q)
    slots[0, block_rows(s), columns(t)] = send[s, 0]
    slots[1, block_rows(s), columns(t)] = send[s, 1]

    pl.semaphore_wait(barrier, len(peers))

    def block(src, tt):
        return slots.at[:, block_rows(src), columns(tt)]

    turns = [(0, 1)]
    for i in range(1, nz - 1, 2):
        turns += [(i, 0), (i + 1, 0), (i, 1), (i + 1, 1)]
    turns += [(nz - 1, 0), (nz - 1, 1)]
    sent = []

    def send_next():
        if len(sent) < len(turns):
            i, e = turns[len(sent)]
            to = member(i, e)
            copy = remote(send.at[to], block(s, t), a_send.at[2 * i + e], a_recv.at[s], (to, t))
            copy.start()
            sent.append(copy)

    for _ in range(AHEAD):
        send_next()

    def at(zz):
        return lax.rem(zz + 2 * nz, nz) * 2 + x

    def hop(j, sign, send_sem, recv_sem, source):
        held = at(z - sign * j)
        return go(
            remote(
                source, kept_out.at[held], send_sem.at[j], recv_sem.at[j], (at(z + sign), t)
            ),
            "wait_send",
        )

    kept_moving = []

    def across(held, index, source):
        kept_moving.append(
            go(
                remote(
                    source, kept_out.at[held], x_send.at[index], x_recv.at[index],
                    (z * 2 + 1 - x, t),
                ),
                "wait_send",
            )
        )

    right_steps, left_steps = nz // 2, nz - 1 - nz // 2
    moving = {}

    def kept_start():
        if right_steps:
            moving["right"] = hop(0, 1, r_send, r_recv, kept_ref)
        if left_steps:
            moving["left"] = hop(0, -1, l_send, l_recv, kept_ref)

    def kept_relay(j):
        if j <= right_steps:
            moving["right"].wait_recv()
            held = at(z - j)
            if j < right_steps:
                moving["right"] = hop(j, 1, r_send, r_recv, kept_out.at[held])
            across(held, 2 * j - 1, kept_out.at[held])
        if j <= left_steps:
            moving["left"].wait_recv()
            held = at(z + j)
            if j < left_steps:
                moving["left"] = hop(j, -1, l_send, l_recv, kept_out.at[held])
            across(held, 2 * j, kept_out.at[held])

    from_far, from_partner = {}, {}

    def arrive(i, e):
        src = member(i, e)
        mine = block(src, t)
        if (i, e) != (0, 0):
            remote(
                send.at[src], mine, a_send.at[2 * i + e], a_recv.at[src], (src, t)
            ).wait_recv()
        k = 2 * i + e
        for d in range(1, ny):
            from_far[d, k] = go(
                remote(mine, mine, y_send.at[d, k], y_recv.at[d, k], away(d)), "wait_send"
            )
        from_partner[0, k] = go(
            remote(mine, mine, p_send.at[0, k], p_recv.at[0, k], partner), "wait_send"
        )
        if k:
            sent[turns.index((i, e))].wait_send()
            send_next()

    def relay(i, e):
        k = 2 * i + e
        for d in range(1, ny):
            from_far[d, k].wait_recv()
            theirs = block(member(i, e), lax.rem(y - d + ny, ny) * 2 + c)
            from_partner[d, k] = go(
                remote(theirs, theirs, p_send.at[d, k], p_recv.at[d, k], partner), "wait_send"
            )

    across_dims = (((1,), (1,)), ((), ()))
    along_dims = (((0,), (0,)), ((), ()))

    units = [(i, None) for i in range(nz - 1)] + [(nz - 1, 0), (nz - 1, 1)]

    def unit_rows(u):
        i, e = units[u]
        return chunk_rows(i) if e is None else block_rows(member(i, e))

    def unit_blocks(u):
        i, e = units[u]
        return [(i, 0), (i, 1)] if e is None else [(i, e)]

    def expert(u):
        for i, e in unit_blocks(u):
            for d in range(ny):
                from_partner[d, 2 * i + e].wait_recv()
        r = unit_rows(u)
        gate = jnp.dot(slots[0, r, :], gate_w[...], preferred_element_type=F32)
        up = jnp.dot(slots[0, r, :], up_w[...], preferred_element_type=F32)
        act_grad = lax.dot_general(
            slots[1, r, :], down_w[...], across_dims, preferred_element_type=F32
        )
        sig = jax.nn.sigmoid(gate)
        swish = gate * sig
        act[r, :] = (swish * up).astype(BF16)
        gate_grad = (act_grad * up * sig * (1.0 + gate * (1.0 - sig))).astype(BF16)
        up_grad = (act_grad * swish).astype(BF16)
        both_grads[r, pl.ds(0, width)] = gate_grad
        both_grads[r, pl.ds(width, width)] = up_grad
        part[r, :] = (
            lax.dot_general(gate_grad, gate_w[...], across_dims, preferred_element_type=F32)
            + lax.dot_general(up_grad, up_w[...], across_dims, preferred_element_type=F32)
        ).astype(BF16)

    halves, summed, returns = {}, {}, {}

    def swap_halves(u):
        r = unit_rows(u)
        for d in list(range(1, ny)) + [0]:
            theirs = lax.rem(y + d, ny) * 2 + 1 - c
            halves[d, u] = go(
                remote(
                    part.at[r, columns(theirs)], near.at[d, r, :],
                    n_send.at[d, u], n_recv.at[d, u], partner,
                ),
                "wait_send",
            )

    def send_pairs(u):
        r = unit_rows(u)
        for d in range(1, ny):
            halves[d, u].wait_recv()
            tt = lax.rem(y + d, ny) * 2 + c
            pairs[d, r, :] = (
                part[r, columns(tt)].astype(F32) + near[d, r, :].astype(F32)
            ).astype(BF16)
            summed[d, u] = go(
                remote(
                    pairs.at[d, r, :], far.at[d, r, :], f_send.at[d, u], f_recv.at[d, u], (s, tt)
                ),
                "wait_send",
            )

    def send_back(u):
        r = unit_rows(u)
        halves[0, u].wait_recv()
        total = part[r, columns(t)].astype(F32) + near[0, r, :].astype(F32)
        for d in range(1, ny):
            summed[d, u].wait_recv()
            total = total + far[d, r, :].astype(F32)
        share[r, :] = total.astype(BF16)
        for i, e in unit_blocks(u):
            to = member(i, e)
            if (i, e) == (0, 0):
                back[block_rows(s), :] = share[block_rows(s), :]
            else:
                go(
                    remote(
                        share.at[block_rows(to), :], back.at[block_rows(s), :],
                        b_send.at[2 * i + e], b_recv.at[s], (to, t),
                    ),
                    "wait_send",
                )

    def returned(i):
        for e in range(2):
            if (i, e) != (0, 0):
                src = member(i, e)
                remote(
                    share.at[block_rows(src), :], back.at[block_rows(src), :],
                    b_send.at[2 * i + e], b_recv.at[src], (src, t),
                ).wait_recv()
        r = chunk_rows(i)
        return lax.dot_general(
            pick[r, :], back[r, :], along_dims, preferred_element_type=F32
        )

    def down_grads():
        turned = act[...].T
        wide = 512
        for j in range(0, down_grad_ref.shape[2], wide):
            down_grad_ref[0, :, j : j + wide] = jnp.dot(
                turned, slots[1, :, j : j + wide], preferred_element_type=F32
            ).astype(BF16)

    def in_grads(lo, hi):
        tall = 256

        def step(j, carry):
            band = pl.ds(pl.multiple_of(j * tall, tall), tall)
            grads = lax.dot_general(
                slots[0, :, band], both_grads[...], along_dims, preferred_element_type=F32
            ).astype(BF16)
            gate_grad_ref[0, band, :] = grads[:, :width]
            up_grad_ref[0, band, :] = grads[:, width:]
            return carry

        count = gate_grad_ref.shape[1] // tall
        lax.fori_loop(lo * count // 4, hi * count // 4, step, 0)

    ends_moving = []
    for k in range(1, n):
        to = lax.rem(s + k, n)
        ends_moving.append(
            go(
                remote(ends_out.at[s], ends_out.at[s], e_send.at[k], e_recv.at[k], (to, t)),
                "wait_send",
            )
        )
    def loaded():
        for copy in loads[6:]:
            copy.wait()

    def forward(i):
        relay(i, 0)
        relay(i, 1)

    def work(u):
        expert(u)
        swap_halves(u)

    arrive(0, 0)
    arrive(0, 1)
    loaded()
    kept_out[s] = kept_ref[...]
    across(s, 0, kept_ref)
    last = nz - 1
    for i in range(1, last, 2):
        arrive(i, 0)
        arrive(i + 1, 0)
        if i == 1:
            forward(0)
        arrive(i, 1)
        if i == 1:
            work(0)
        else:
            forward(i - 1)
            send_pairs(i - 2)
            work(i - 1)
            send_back(i - 3)
        arrive(i + 1, 1)
        forward(i)
        send_pairs(i - 1)
        work(i)
        if i > 1:
            send_back(i - 2)
    arrive(last, 0)
    forward(last - 1)
    send_pairs(last - 2)
    arrive(last, 1)
    kept_start()
    work(last - 1)
    if last > 2:
        send_back(last - 3)
    relay(last, 0)
    send_pairs(last - 1)
    work(last)
    send_back(last - 2)
    relay(last, 1)
    send_pairs(last)
    kept_relay(1)
    work(last + 1)
    send_back(last - 1)
    send_pairs(last + 1)
    send_back(last)
    down_grads()
    send_back(last + 1)
    in_grads(0, 2)
    token = returned(0)
    for i in range(1, nz):
        token = token + returned(i)
    stream_ref[:, columns(t)] = (grad_ref[...].astype(F32) + token).astype(BF16)
    mine = stream_ref.at[:, columns(t)]
    outer = {}
    for d in range(1, ny):
        outer[d] = go(remote(mine, mine, g_send.at[d], g_recv.at[d], away(d)), "wait_send")
    inner = {}
    inner[0] = go(remote(mine, mine, h_send.at[0], h_recv.at[0], partner), "wait_send")
    in_grads(2, 4)
    for j in range(2, nz):
        kept_relay(j)
    value_dim, key_dim = value_ref.shape[1] // heads, key_ref.shape[1] // heads
    def expand(rows, width, depth):
        lane = lax.div(lax.broadcasted_iota(jnp.int32, (rows[0].shape[0], width), 1), depth)
        out = jnp.zeros((rows[0].shape[0], width), F32)
        for h in range(heads):
            out = jnp.where(lane == h, jnp.broadcast_to(rows[h], out.shape), out)
        return out

    key_width, value_width = heads * key_dim, heads * value_dim
    exact = lax.Precision.HIGHEST
    low = (first >= second).astype(F32)
    total = lax.dot_general(
        low, decay_ref[...], across_dims, precision=exact, preferred_element_type=F32
    )
    total_row = lax.dot_general(
        decay_ref[...], low, across_dims, precision=exact, preferred_element_type=F32
    )
    head_total = [total[:, h : h + 1] for h in range(heads)]
    head_row = [total_row[h : h + 1, :] for h in range(heads)]
    head_end = [total[tokens - 1 : tokens, h : h + 1] for h in range(heads)]
    grown = jnp.exp(expand(head_total, key_width, key_dim))
    state_row = lax.div(lax.broadcasted_iota(jnp.int32, (key_width, value_width), 0), key_dim)
    state_lane = lax.div(lax.broadcasted_iota(jnp.int32, (key_width, value_width), 1), value_dim)
    diagonal = state_row == state_lane
    for copy in ends_moving:
        copy.wait_recv()
    before = [jnp.zeros((1, value_width), F32)]
    since = jnp.zeros((1, value_width), F32)
    for b in range(n):
        ends = expand([ends_out[b, h : h + 1, 0:1] for h in range(heads)], value_width, value_dim)
        before.append(before[-1] + ends)
        since = since + ends * below(b, 2 * z + 2, 2 * n).astype(F32)
    for zz in range(nz):
        reach[zz] = jnp.broadcast_to(
            jnp.exp(jnp.minimum(before[2 * zz] - since, 0.0))
            * below(z, zz, nz).astype(F32),
            (8, value_width),
        )

    def state_ends(b):
        return expand(
            [ends_out[b, h : h + 1, 0:1] for h in range(heads)], value_width, value_dim
        )

    lower = (1 - x).astype(F32)
    half = key_dim // 2

    key_lane = lax.div(lax.broadcasted_iota(jnp.int32, (tokens, key_width), 1), key_dim)
    value_lane = lax.div(lax.broadcasted_iota(jnp.int32, (tokens, value_width), 1), value_dim)

    def only(values, lane, h):
        return jnp.where(lane == h, values, jnp.zeros_like(values))

    place = lax.broadcasted_iota(jnp.int32, (value_dim, value_width), 0)
    spot = lax.broadcasted_iota(jnp.int32, (value_dim, value_width), 1)
    for h in range(heads):
        put = (place + h * value_dim == spot).astype(F32).astype(BF16)
        incoming[h * key_dim : (h + 1) * key_dim, :] = jnp.dot(
            incoming_ref[0, h].astype(BF16), put, preferred_element_type=F32
        ).astype(BF16)
    for h in range(heads):
        diff = head_total[h] - head_row[h]
        fade[h] = jnp.where(first >= second, jnp.exp(jnp.minimum(diff, 0.0)), 0.0)
        fade_turned[h] = jnp.where(first <= second, jnp.exp(jnp.minimum(-diff, 0.0)), 0.0)
        pointed = lax.dot_general(
            only(key_ref[...], key_lane, h), query_ref[...], across_dims,
            preferred_element_type=F32,
        )
        score[h] = (pointed * fade_turned[h]).astype(BF16)
    for d in range(1, ny):
        outer[d].wait_recv()
        theirs = stream_ref.at[:, columns(lax.rem(y - d + ny, ny) * 2 + c)]
        inner[d] = go(
            remote(theirs, theirs, h_send.at[d], h_recv.at[d], partner), "wait_send"
        )
    band_count = 2 * ny if tokens % (32 * ny) == 0 else 2
    tall = tokens // band_count
    wide = cols_ref.shape[2]
    tp_bands = band_count > 2

    def band(yy, cc):
        return pl.ds(pl.multiple_of((yy * 2 + cc if tp_bands else cc) * tall, tall), tall)

    ret = lax.dot_general(
        stream_ref[:, columns(t)], proj[:, columns(t)], across_dims, preferred_element_type=F32
    )
    for d in range(1, ny):
        tt = lax.rem(y - d + ny, ny) * 2 + c
        ret = ret + lax.dot_general(
            stream_ref[:, columns(tt)], proj[:, columns(tt)], across_dims,
            preferred_element_type=F32,
        )
    for d in range(ny):
        inner[d].wait_recv()

    def piece(b, rows):
        if wide % 128:
            return blocks.at[b, rows]
        return stream_ref.at[rows, pl.ds(pl.multiple_of(b * wide, wide), wide)]

    if wide % 128:
        for b in range(n):
            blocks[b] = stream_ref[:, b * wide : (b + 1) * wide]

    def send_columns(i, e):
        to = member(i, e)
        go(
            remote(
                piece(to, band(y, c)), cols_ref.at[s, band(y, c)],
                c_send.at[2 * i + e], c_recv.at[s], (to, t),
            ),
            "wait_send",
        )

    for i, e in turns:
        send_columns(i, e)
    for d in range(ny):
        tt = lax.rem(y - d + ny, ny) * 2 + 1 - c
        ret = ret + lax.dot_general(
            stream_ref[:, columns(tt)], proj[:, columns(tt)], across_dims,
            preferred_element_type=F32,
        )
    o_ref[...] = ret.astype(BF16)

    injected = lax.dot_general(
        (query_ref[...].astype(F32) * grown).astype(BF16), o_ref[...], along_dims,
        preferred_element_type=F32,
    )
    injected = jnp.where(diagonal, injected, 0.0)
    folded = injected[:key_dim, :]
    for h in range(1, heads):
        folded = folded + injected[h * key_dim : (h + 1) * key_dim, :]
    own_state[...] = folded.astype(BF16)
    pair_copy = go(
        remote(own_state, pair_state, u_send.at[0], u_recv.at[0], (z * 2 + 1 - x, t)),
        "wait_send",
    )
    cols_ref[s] = piece(s, pl.ds(0, tokens))[...]

    query_grad = grown * lax.dot_general(
        o_ref[...], incoming[...], across_dims, preferred_element_type=F32
    )
    key_grad = jnp.zeros((tokens, key_width), F32)
    value_grad = jnp.zeros((tokens, value_width), F32)
    def head_grads(h, grads):
        query_grad, key_grad, value_grad = grads
        o_head = only(o_ref[...], value_lane, h)
        v_head = only(value_ref[...], value_lane, h)
        q_head = only(query_ref[...], key_lane, h)
        k_head = only(key_ref[...], key_lane, h)
        prob = lax.dot_general(o_head, value_ref[...], across_dims, preferred_element_type=F32)
        query_grad = query_grad + jnp.dot(
            (prob * fade[h]).astype(BF16), k_head, preferred_element_type=F32
        )
        prob = lax.dot_general(v_head, o_ref[...], across_dims, preferred_element_type=F32)
        key_grad = key_grad + jnp.dot(
            (prob * fade_turned[h]).astype(BF16), q_head, preferred_element_type=F32
        )
        value_grad = value_grad + jnp.dot(score[h], o_head, preferred_element_type=F32)
        return query_grad, key_grad, value_grad

    from_far, joined = {}, {}

    def columns_arrive(i, e):
        src, k = member(i, e), 2 * i + e
        mine = cols_ref.at[src, band(y, c)]
        remote(
            piece(src, band(y, c)), mine, c_send.at[k], c_recv.at[src], (src, t)
        ).wait_recv()
        if tp_bands:
            for d in range(1, ny):
                from_far[d, k] = go(
                    remote(mine, mine, v_send.at[d, k], v_recv.at[d, k], away(d)), "wait_send"
                )
        joined[0, k] = go(
            remote(mine, mine, w_send.at[0, k], w_recv.at[0, k], partner), "wait_send"
        )

    grads = (query_grad, key_grad, value_grad)
    for h in range(heads // 2):
        grads = head_grads(h, grads)
    pair_copy.wait_recv()
    mine, other = own_state[...].astype(F32), pair_state[...].astype(F32)
    both = lower * mine + (1.0 - lower) * other + jnp.exp(state_ends(z * 2)) * (
        lower * other + (1.0 - lower) * mine
    )
    both_halves[0] = both[:half].astype(BF16)
    both_halves[1] = both[half:].astype(BF16)
    for i in range(1, nz):
        go(
            remote(
                both_halves.at[x], states.at[z], s_send.at[i], s_recv.at[z], (order[i] * 2 + x, t)
            ),
            "wait_send",
        )
    for i, e in turns[:3]:
        columns_arrive(i, e)
    for h in range(heads // 2, heads):
        grads = head_grads(h, grads)
    query_grad, key_grad, value_grad = grads
    query_out[...] = query_grad.astype(BF16)

    def gather(i):
        for e in range(2):
            for d in range(ny if tp_bands else 1):
                if (d, 2 * i + e) in joined:
                    joined[d, 2 * i + e].wait_recv()
        pair = pl.ds(order[i] * 2, 2)
        added = lax.dot_general(
            cols_ref[pair].reshape(2 * tokens, wide),
            kept_out[pair].reshape(2 * tokens, kept_ref.shape[1]),
            along_dims, preferred_element_type=F32,
        )
        if i == 0:
            proj_grad[...] = added
        else:
            proj_grad[...] += added

    for i, e in turns[3:5]:
        columns_arrive(i, e)
    later = jnp.zeros((half, value_width), F32)
    for i in range(1, nz):
        src = order[i]
        remote(
            both_halves.at[x], states.at[src], s_send.at[i], s_recv.at[src], (src * 2 + x, t)
        ).wait_recv()
        later = later + reach[src][0:1, :] * states[src].astype(F32)
    later_halves[x] = later.astype(BF16)
    turned = go(
        remote(
            later_halves.at[x], later_halves.at[x], u_send.at[1], u_recv.at[1],
            (z * 2 + 1 - x, t),
        ),
        "wait_send",
    )
    for i, e in turns[5:]:
        columns_arrive(i, e)
    for copy in kept_moving:
        copy.wait_recv()
    turned.wait_recv()
    later = jnp.concatenate([later_halves[j].astype(F32) for j in range(2)], axis=0)
    later = jnp.exp(lower * state_ends(z * 2 + 1)) * later + lower * pair_state[...].astype(F32)
    stacked = jnp.concatenate([later.astype(BF16)] * heads, axis=0)
    stacked = jnp.where(diagonal, stacked, jnp.zeros_like(stacked))
    left = [end - own for end, own in zip(head_end, head_total)]
    key_grad = key_grad + jnp.exp(expand(left, key_width, key_dim)) * lax.dot_general(
        value_ref[...], stacked, across_dims, preferred_element_type=F32
    )
    key_out[...] = key_grad.astype(BF16)
    value_grad = value_grad + jnp.exp(expand(left, value_width, value_dim)) * jnp.dot(
        key_ref[...], stacked, preferred_element_type=F32
    )
    value_out[...] = value_grad.astype(BF16)
    for i in range(nz):
        for e in range(2):
            if (i, e) == (0, 0):
                continue
            src, k = member(i, e), 2 * i + e
            if tp_bands:
                for d in range(1, ny):
                    from_far[d, k].wait_recv()
                    theirs = cols_ref.at[src, band(lax.rem(y - d + ny, ny), c)]
                    joined[d, k] = go(
                        remote(theirs, theirs, w_send.at[d, k], w_recv.at[d, k], partner),
                        "wait_send",
                    )
        if i:
            gather(i - 1)
    gather(nz - 1)
    for wait in waits:
        wait()


def main_part(
    n, ny, cap, ids, weights, decay, rows, grad, kept, gate_w, up_w, down_w, proj, query, key,
    value, incoming,
):
    tokens, q = grad.shape
    heads = decay.shape[0]
    dma = pltpu.SemaphoreType.DMA
    slots, model, width = n * cap, rows.shape[1], gate_w.shape[2]
    nz = n // 2
    state = (key.shape[1] // heads, value.shape[1])
    half_state = (state[0] // 2, state[1])
    vmem = pl.BlockSpec(memory_space=pltpu.VMEM)
    return pl.pallas_call(
        functools.partial(main_kernel, n, ny, cap),
        out_shape=(
            jax.ShapeDtypeStruct((model // n, kept.shape[1]), F32),
            jax.ShapeDtypeStruct(gate_w.shape, BF16),
            jax.ShapeDtypeStruct(up_w.shape, BF16),
            jax.ShapeDtypeStruct(down_w.shape, BF16),
            jax.ShapeDtypeStruct(query.shape, BF16),
            jax.ShapeDtypeStruct(key.shape, BF16),
            jax.ShapeDtypeStruct(value.shape, BF16),
        ),
        in_specs=[pl.BlockSpec(memory_space=pltpu.HBM)] * 14,
        out_specs=[vmem] * 7,
        scratch_shapes=[
            pltpu.VMEM((n,) + kept.shape, BF16),
            pltpu.VMEM((n, tokens, model // n), BF16),
            pltpu.VMEM((tokens, model), BF16),
            pltpu.VMEM((n, 8, 128), F32),
            pltpu.VMEM(proj.shape, BF16),
            pltpu.VMEM((key.shape[1], value.shape[1]), BF16),
            pltpu.VMEM((tokens, value.shape[1]), BF16),
            pltpu.VMEM((nz,) + half_state, BF16),
            pltpu.VMEM(state, BF16),
            pltpu.VMEM(state, BF16),
            pltpu.VMEM((nz, 8, value.shape[1]), F32),
            pltpu.VMEM((2,) + half_state, BF16),
            pltpu.VMEM((2,) + half_state, BF16),
            pltpu.VMEM((n, tokens, model // n) if model // n % 128 else (1, 8, 128), BF16),
            pltpu.VMEM((heads, tokens, tokens), F32),
            pltpu.VMEM((heads, tokens, tokens), F32),
            pltpu.VMEM((heads, tokens, tokens), BF16),
            pltpu.VMEM(ids.shape, jnp.int32),
            pltpu.VMEM(weights.shape, F32),
            pltpu.VMEM(decay.shape, F32),
            pltpu.VMEM(grad.shape, BF16),
            pltpu.VMEM(kept.shape, BF16),
            pltpu.VMEM(query.shape, BF16),
            pltpu.VMEM(key.shape, BF16),
            pltpu.VMEM(value.shape, BF16),
            pltpu.VMEM(incoming.shape, F32),
            pltpu.VMEM((tokens, q), BF16),
            pltpu.VMEM(gate_w.shape[1:], BF16),
            pltpu.VMEM(up_w.shape[1:], BF16),
            pltpu.VMEM(down_w.shape[1:], BF16),
            pltpu.VMEM((slots, tokens), BF16),
            pltpu.VMEM((n, 2, cap, q), BF16),
            pltpu.VMEM((2, slots, model), BF16),
            pltpu.VMEM((slots, width), BF16),
            pltpu.VMEM((slots, 2 * width), BF16),
            pltpu.VMEM((slots, model), BF16),
            pltpu.VMEM((ny, slots, q), BF16),
            pltpu.VMEM((ny, slots, q), BF16),
            pltpu.VMEM((ny, slots, q), BF16),
            pltpu.VMEM((slots, q), BF16),
            pltpu.VMEM((slots, q), BF16),
            dma((14,)),
        ]
        + [dma((n,))] * 4
        + [dma((ny, n))] * 4
        + [dma((ny, nz + 1))] * 4
        + [dma((n,))] * 2
        + [dma((ny,))] * 4
        + [dma((n,))] * 6
        + [dma((nz,))] * 2
        + [dma((2,))] * 2
        + [dma((n,))] * 2
        + [dma((ny, n))] * 4,
        compiler_params=pltpu.CompilerParams(
            collective_id=0, has_side_effects=True, vmem_limit_bytes=LIMIT
        ),
    )(
        *(
            pltpu.with_memory_space_constraint(array, pltpu.HBM)
            for array in (
                ids, weights, decay, rows, grad, kept, gate_w, up_w, down_w, proj, query, key,
                value, incoming,
            )
        )
    )


def final_kernel(*refs):
    moved = len(refs) // 2
    copies = [
        pltpu.make_async_copy(source, target, refs[-1].at[j])
        for j, (source, target) in enumerate(zip(refs[:moved], refs[moved:-1]))
    ]
    for copy in copies:
        copy.start()
    for copy in copies:
        copy.wait()


def final_part(*moved):
    return pl.pallas_call(
        final_kernel,
        out_shape=tuple(jax.ShapeDtypeStruct(array.shape, array.dtype) for array in moved),
        in_specs=[pl.BlockSpec(memory_space=pltpu.VMEM)] * len(moved),
        out_specs=[pl.BlockSpec(memory_space=pltpu.HBM)] * len(moved),
        scratch_shapes=[pltpu.SemaphoreType.DMA((len(moved),))],
        compiler_params=pltpu.CompilerParams(vmem_limit_bytes=LIMIT // 4),
    )(*moved)


def on_device(
    moe_input,
    out_grad,
    expert_ids,
    expert_weights,
    w_gate,
    w_up,
    w_down,
    out_proj,
    retained,
    queries,
    keys,
    values,
    log_decay,
    incoming_state,
):
    n, ny = lax.axis_size("sp"), lax.axis_size("tp") // 2
    tokens_here = moe_input.shape[0]
    capacity = -(-(5 * tokens_here // (2 * n)) // 16) * 16
    proj_grad, gate_grad, up_grad, down_grad, query_grad, key_grad, value_grad = final_part(
        *main_part(
            n, ny, capacity, expert_ids.T, expert_weights.T, log_decay.T, moe_input, out_grad,
            retained, w_gate, w_up, w_down, out_proj, queries, keys, values, incoming_state,
        )
    )
    return gate_grad, up_grad, down_grad, proj_grad, query_grad, key_grad, value_grad


def solution(mesh):
    placed = (
        P("sp", None),
        P("sp", "tp"),
        P("sp", None),
        P("sp", None),
        P("sp", None, "tp"),
        P("sp", None, "tp"),
        P("sp", "tp", None),
        P("tp", None),
        P("sp", "tp"),
        P("sp", "tp"),
        P("sp", "tp"),
        P("sp", "tp"),
        P("sp", "tp"),
        P("sp", "tp", None, None),
    )
    return jax.shard_map(
        on_device,
        mesh=mesh,
        in_specs=placed,
        out_specs=(
            P("sp", None, "tp"),
            P("sp", None, "tp"),
            P("sp", "tp", None),
            P("sp", "tp"),
            P("sp", "tp"),
            P("sp", "tp"),
            P("sp", "tp"),
        ),
        check_vma=False,
    )
```

```python
import functools

import jax
import jax.numpy as jnp
from jax import lax
from jax.experimental import pallas as pl
from jax.experimental.pallas import tpu as pltpu
from jax.sharding import PartitionSpec as P

MESH = pl.DeviceIdType.MESH
F32 = jnp.float32
BF16 = jnp.bfloat16
LIMIT = 38 * 1024 * 1024
AHEAD = 5


def where_am_i(n, ny):
    s, t = lax.axis_index("sp"), lax.axis_index("tp")
    return s, t, lax.div(t, 2), lax.rem(t, 2)


def greet(peers):
    barrier = pltpu.get_barrier_semaphore()
    for peer in peers:
        pl.semaphore_signal(barrier, inc=1, device_id=peer, device_id_type=MESH)
    pl.semaphore_wait(barrier, len(peers))


def sp_peers(n, s, t):
    return [(lax.rem(s + k, n), t) for k in range(1, n)]


def tp_peers(ny, s, y, c):
    return [(s, lax.rem(y + d, ny) * 2 + c) for d in range(1, ny)] + [(s, y * 2 + 1 - c)]


def remote(src, dst, send, recv, peer):
    return pltpu.make_async_remote_copy(
        src_ref=src, dst_ref=dst, send_sem=send, recv_sem=recv, device_id=peer, device_id_type=MESH
    )


def below(a, b, top):
    return lax.div(b - a + top - 1, top)


def flipped(z, i, nz):
    if nz & (nz - 1):
        return lax.rem(z + i, nz)
    out, bit = 0, 1
    while bit < nz:
        own = lax.rem(lax.div(z, bit), 2)
        out = out + bit * (1 - own if i & bit else own)
        bit *= 2
    return out


def main_kernel(
    n, ny, cap, ids_hbm, weights_hbm, decay_hbm, rows_hbm, grad_hbm, kept_hbm,
    gate_hbm, up_hbm, down_hbm, proj_hbm, query_hbm, key_hbm, value_hbm, incoming_hbm,
    proj_grad, gate_grad_ref, up_grad_ref, down_grad_ref, query_out, key_out, value_out,
    kept_out, cols_ref, stream_ref, ends_out, proj, incoming, o_ref, states, own_state, pair_state, reach, both_state,

    blocks, fade, fade_turned, score, ids_ref, weights_ref, decay_ref, grad_ref, kept_ref, query_ref, key_ref, value_ref,
    incoming_ref, rows_v, gate_w, up_w, down_w, pick, send, slots, act, both_grads, part, near, pairs, far,
    share, back,
    load_sem, a_send, a_recv, e_send, e_recv, y_send, y_recv, p_send, p_recv,
    n_send, n_recv, f_send, f_recv, b_send, b_recv, g_send, g_recv, h_send, h_recv,
    r_send, r_recv, l_send, l_recv, x_send, x_recv,
    s_send, s_recv, u_send, u_recv, c_send, c_recv, v_send, v_recv, w_send, w_recv,
):
    s, t, y, c = where_am_i(n, ny)
    tokens, q = grad_ref.shape
    heads = decay_ref.shape[0]
    width = gate_w.shape[1]
    nz = n // 2
    z, x = lax.div(s, 2), lax.rem(s, 2)
    partner = (s, y * 2 + 1 - c)
    order = [flipped(z, i, nz) for i in range(nz)]
    waits = []

    def columns(tt):
        return pl.ds(pl.multiple_of(tt * q, q), q)

    def block_rows(b):
        return pl.ds(pl.multiple_of(b * cap, cap), cap)

    def chunk_rows(i):
        return pl.ds(pl.multiple_of(order[i] * 2 * cap, 2 * cap), 2 * cap)

    def member(i, e):
        return order[i] * 2 + (x if e == 0 else 1 - x)

    def away(d):
        return (s, lax.rem(y + d, ny) * 2 + c)

    def go(copy, wait):
        copy.start()
        waits.append(getattr(copy, wait))
        return copy

    barrier = pltpu.get_barrier_semaphore()
    peers = sp_peers(n, s, t) + tp_peers(ny, s, y, c)
    for peer in peers:
        pl.semaphore_signal(barrier, inc=1, device_id=peer, device_id_type=MESH)

    loads = [
        pltpu.make_async_copy(hbm, local, load_sem.at[j])
        for j, (hbm, local) in enumerate(
            [
                (ids_hbm, ids_ref), (weights_hbm, weights_ref), (decay_hbm, decay_ref),
                (grad_hbm, grad_ref), (rows_hbm.at[:, columns(t)], rows_v), (kept_hbm, kept_ref),
                (gate_hbm.at[0], gate_w), (up_hbm.at[0], up_w), (down_hbm.at[0], down_w),
                (proj_hbm, proj), (query_hbm, query_ref), (key_hbm, key_ref),
                (value_hbm, value_ref), (incoming_hbm, incoming_ref),
            ]
        )
    ]
    for copy in loads:
        copy.start()
    for copy in loads[:3]:
        copy.wait()

    ids = ids_ref[...].astype(F32)
    ids = [ids[j : j + 1, :] for j in range(2)]
    weights = [weights_ref[j : j + 1, :] for j in range(2)]
    expert_row = lax.broadcasted_iota(jnp.int32, (n, tokens), 0).astype(F32)
    named = [(expert_row == own).astype(F32) for own in ids]
    first = lax.broadcasted_iota(jnp.int32, (tokens, tokens), 0)
    second = lax.broadcasted_iota(jnp.int32, (tokens, tokens), 1)
    earlier = jnp.dot(
        (named[0] + named[1]).astype(BF16),
        (first < second).astype(F32).astype(BF16),
        preferred_element_type=F32,
    )
    slot = [
        own * cap + jnp.sum(hot * earlier, axis=0, keepdims=True) for own, hot in zip(ids, named)
    ]
    number = lax.broadcasted_iota(jnp.int32, (n * cap, tokens), 0).astype(F32)
    hits = [(number == own).astype(F32) for own in slot]
    picker = (hits[0] + hits[1]).astype(BF16)
    slot_weight = jnp.sum(hits[0] * weights[0] + hits[1] * weights[1], axis=1, keepdims=True)
    pick[...] = picker
    ends_out[s, :, :] = jnp.zeros((8, 128), F32)
    ends_out[s, pl.ds(0, heads), :] = jnp.broadcast_to(
        jnp.sum(decay_ref[...], axis=1, keepdims=True), (heads, 128)
    )
    for copy in loads[3:5]:
        copy.wait()
    cotangent = jnp.dot(picker, grad_ref[...], preferred_element_type=F32) * slot_weight
    send[:, 1] = cotangent.astype(BF16).reshape(n, cap, q)
    picked = jnp.dot(picker, rows_v[...], preferred_element_type=F32).astype(BF16)
    send[:, 0] = picked.reshape(n, cap, q)
    slots[0, block_rows(s), columns(t)] = send[s, 0]
    slots[1, block_rows(s), columns(t)] = send[s, 1]

    pl.semaphore_wait(barrier, len(peers))

    def block(src, tt):
        return slots.at[:, block_rows(src), columns(tt)]

    turns = [(0, 1)]
    for i in range(1, nz - 1, 2):
        turns += [(i, 0), (i + 1, 0), (i, 1), (i + 1, 1)]
    turns += [(nz - 1, 0), (nz - 1, 1)]
    sent = []

    def send_next():
        if len(sent) < len(turns):
            i, e = turns[len(sent)]
            to = member(i, e)
            copy = remote(send.at[to], block(s, t), a_send.at[2 * i + e], a_recv.at[s], (to, t))
            copy.start()
            sent.append(copy)

    for _ in range(AHEAD):
        send_next()

    def at(zz):
        return lax.rem(zz + 2 * nz, nz) * 2 + x

    def hop(j, sign, send_sem, recv_sem, source):
        held = at(z - sign * j)
        return go(
            remote(
                source, kept_out.at[held], send_sem.at[j], recv_sem.at[j], (at(z + sign), t)
            ),
            "wait_send",
        )

    kept_moving = []

    def across(held, index, source):
        kept_moving.append(
            go(
                remote(
                    source, kept_out.at[held], x_send.at[index], x_recv.at[index],
                    (z * 2 + 1 - x, t),
                ),
                "wait_send",
            )
        )

    right_steps, left_steps = nz // 2, nz - 1 - nz // 2
    moving = {}

    def kept_start():
        if right_steps:
            moving["right"] = hop(0, 1, r_send, r_recv, kept_ref)
        if left_steps:
            moving["left"] = hop(0, -1, l_send, l_recv, kept_ref)

    def kept_relay(j):
        if j <= right_steps:
            moving["right"].wait_recv()
            held = at(z - j)
            across(held, 2 * j - 1, kept_out.at[held])
        if j <= left_steps:
            moving["left"].wait_recv()
            held = at(z + j)
            across(held, 2 * j, kept_out.at[held])

    def kept_onward(j):
        if j < right_steps:
            moving["right"] = hop(j, 1, r_send, r_recv, kept_out.at[at(z - j)])
        if j < left_steps:
            moving["left"] = hop(j, -1, l_send, l_recv, kept_out.at[at(z + j)])

    from_far, from_partner = {}, {}

    def arrive(i, e):
        src = member(i, e)
        mine = block(src, t)
        if (i, e) != (0, 0):
            remote(
                send.at[src], mine, a_send.at[2 * i + e], a_recv.at[src], (src, t)
            ).wait_recv()
        k = 2 * i + e
        for d in range(1, ny):
            from_far[d, k] = go(
                remote(mine, mine, y_send.at[d, k], y_recv.at[d, k], away(d)), "wait_send"
            )
        from_partner[0, k] = go(
            remote(mine, mine, p_send.at[0, k], p_recv.at[0, k], partner), "wait_send"
        )
        if k:
            sent[turns.index((i, e))].wait_send()
            send_next()

    def relay(i, e):
        k = 2 * i + e
        for d in range(1, ny):
            from_far[d, k].wait_recv()
            theirs = block(member(i, e), lax.rem(y - d + ny, ny) * 2 + c)
            from_partner[d, k] = go(
                remote(theirs, theirs, p_send.at[d, k], p_recv.at[d, k], partner), "wait_send"
            )

    across_dims = (((1,), (1,)), ((), ()))
    along_dims = (((0,), (0,)), ((), ()))

    units = [(i, None) for i in range(nz - 1)] + [(nz - 1, 0), (nz - 1, 1)]

    def unit_rows(u):
        i, e = units[u]
        return chunk_rows(i) if e is None else block_rows(member(i, e))

    def unit_blocks(u):
        i, e = units[u]
        return [(i, 0), (i, 1)] if e is None else [(i, e)]

    def expert(u):
        for i, e in unit_blocks(u):
            for d in range(ny):
                from_partner[d, 2 * i + e].wait_recv()
        r = unit_rows(u)
        gate = jnp.dot(slots[0, r, :], gate_w[...], preferred_element_type=F32)
        up = jnp.dot(slots[0, r, :], up_w[...], preferred_element_type=F32)
        act_grad = lax.dot_general(
            slots[1, r, :], down_w[...], across_dims, preferred_element_type=F32
        )
        sig = jax.nn.sigmoid(gate)
        swish = gate * sig
        act[r, :] = (swish * up).astype(BF16)
        gate_grad = (act_grad * up * sig * (1.0 + gate * (1.0 - sig))).astype(BF16)
        up_grad = (act_grad * swish).astype(BF16)
        both_grads[r, pl.ds(0, width)] = gate_grad
        both_grads[r, pl.ds(width, width)] = up_grad
        part[r, :] = (
            lax.dot_general(gate_grad, gate_w[...], across_dims, preferred_element_type=F32)
            + lax.dot_general(up_grad, up_w[...], across_dims, preferred_element_type=F32)
        ).astype(BF16)

    halves, summed, returns = {}, {}, {}

    def swap_halves(u):
        r = unit_rows(u)
        for d in list(range(1, ny)) + [0]:
            theirs = lax.rem(y + d, ny) * 2 + 1 - c
            halves[d, u] = go(
                remote(
                    part.at[r, columns(theirs)], near.at[d, r, :],
                    n_send.at[d, u], n_recv.at[d, u], partner,
                ),
                "wait_send",
            )

    def send_pairs(u):
        r = unit_rows(u)
        for d in range(1, ny):
            halves[d, u].wait_recv()
            tt = lax.rem(y + d, ny) * 2 + c
            pairs[d, r, :] = (
                part[r, columns(tt)].astype(F32) + near[d, r, :].astype(F32)
            ).astype(BF16)
            summed[d, u] = go(
                remote(
                    pairs.at[d, r, :], far.at[d, r, :], f_send.at[d, u], f_recv.at[d, u], (s, tt)
                ),
                "wait_send",
            )

    def send_back(u):
        r = unit_rows(u)
        halves[0, u].wait_recv()
        total = part[r, columns(t)].astype(F32) + near[0, r, :].astype(F32)
        for d in range(1, ny):
            summed[d, u].wait_recv()
            total = total + far[d, r, :].astype(F32)
        share[r, :] = total.astype(BF16)
        for i, e in unit_blocks(u):
            to = member(i, e)
            if (i, e) == (0, 0):
                back[block_rows(s), :] = share[block_rows(s), :]
            else:
                go(
                    remote(
                        share.at[block_rows(to), :], back.at[block_rows(s), :],
                        b_send.at[2 * i + e], b_recv.at[s], (to, t),
                    ),
                    "wait_send",
                )

    def returned(i):
        for e in range(2):
            if (i, e) != (0, 0):
                src = member(i, e)
                remote(
                    share.at[block_rows(src), :], back.at[block_rows(src), :],
                    b_send.at[2 * i + e], b_recv.at[src], (src, t),
                ).wait_recv()
        r = chunk_rows(i)
        return lax.dot_general(
            pick[r, :], back[r, :], along_dims, preferred_element_type=F32
        )

    def down_grads():
        turned = act[...].T
        wide = 512
        for j in range(0, down_grad_ref.shape[2], wide):
            down_grad_ref[0, :, j : j + wide] = jnp.dot(
                turned, slots[1, :, j : j + wide], preferred_element_type=F32
            ).astype(BF16)

    def in_grads(lo, hi):
        tall = 256

        def step(j, carry):
            band = pl.ds(pl.multiple_of(j * tall, tall), tall)
            grads = lax.dot_general(
                slots[0, :, band], both_grads[...], along_dims, preferred_element_type=F32
            ).astype(BF16)
            gate_grad_ref[0, band, :] = grads[:, :width]
            up_grad_ref[0, band, :] = grads[:, width:]
            return carry

        count = gate_grad_ref.shape[1] // tall
        lax.fori_loop(lo * count // 4, hi * count // 4, step, 0)

    ends_moving = []
    for k in range(1, n):
        to = lax.rem(s + k, n)
        ends_moving.append(
            go(
                remote(ends_out.at[s], ends_out.at[s], e_send.at[k], e_recv.at[k], (to, t)),
                "wait_send",
            )
        )
    def loaded():
        for copy in loads[5:]:
            copy.wait()

    def forward(i):
        relay(i, 0)
        relay(i, 1)

    def work(u):
        expert(u)
        swap_halves(u)

    arrive(0, 0)
    arrive(0, 1)
    loaded()
    kept_out[s] = kept_ref[...]
    across(s, 0, kept_ref)
    last = nz - 1
    for i in range(1, last, 2):
        arrive(i, 0)
        arrive(i + 1, 0)
        if i == 1:
            forward(0)
        arrive(i, 1)
        if i == 1:
            work(0)
        else:
            forward(i - 1)
            send_pairs(i - 2)
            work(i - 1)
            send_back(i - 3)
        arrive(i + 1, 1)
        forward(i)
        send_pairs(i - 1)
        work(i)
        if i > 1:
            send_back(i - 2)
    arrive(last, 0)
    forward(last - 1)
    arrive(last, 1)
    send_pairs(last - 2)
    kept_start()
    work(last - 1)
    if last > 2:
        send_back(last - 3)
    relay(last, 0)
    send_pairs(last - 1)
    work(last)
    send_back(last - 2)
    relay(last, 1)
    send_pairs(last)
    kept_relay(1)
    send_back(last - 1)
    work(last + 1)
    send_pairs(last + 1)
    send_back(last)
    down_grads()
    send_back(last + 1)
    in_grads(0, 2)
    token = returned(0)
    for i in range(1, nz):
        token = token + returned(i)
    stream_ref[:, columns(t)] = (grad_ref[...].astype(F32) + token).astype(BF16)
    mine = stream_ref.at[:, columns(t)]
    outer = {}
    for d in range(1, ny):
        outer[d] = go(remote(mine, mine, g_send.at[d], g_recv.at[d], away(d)), "wait_send")
    kept_onward(1)
    inner = {}
    inner[0] = go(remote(mine, mine, h_send.at[0], h_recv.at[0], partner), "wait_send")
    in_grads(2, 4)
    value_dim, key_dim = value_ref.shape[1] // heads, key_ref.shape[1] // heads
    def expand(rows, width, depth):
        lane = lax.div(lax.broadcasted_iota(jnp.int32, (rows[0].shape[0], width), 1), depth)
        out = jnp.zeros((rows[0].shape[0], width), F32)
        for h in range(heads):
            out = jnp.where(lane == h, jnp.broadcast_to(rows[h], out.shape), out)
        return out

    key_width, value_width = heads * key_dim, heads * value_dim
    exact = lax.Precision.HIGHEST
    low = (first >= second).astype(F32)
    total = lax.dot_general(
        low, decay_ref[...], across_dims, precision=exact, preferred_element_type=F32
    )
    total_row = lax.dot_general(
        decay_ref[...], low, across_dims, precision=exact, preferred_element_type=F32
    )
    head_total = [total[:, h : h + 1] for h in range(heads)]
    head_row = [total_row[h : h + 1, :] for h in range(heads)]
    head_end = [total[tokens - 1 : tokens, h : h + 1] for h in range(heads)]
    grown = jnp.exp(expand(head_total, key_width, key_dim))
    state_row = lax.div(lax.broadcasted_iota(jnp.int32, (key_width, value_width), 0), key_dim)
    state_lane = lax.div(lax.broadcasted_iota(jnp.int32, (key_width, value_width), 1), value_dim)
    diagonal = state_row == state_lane
    for copy in ends_moving:
        copy.wait_recv()
    before = [jnp.zeros((1, value_width), F32)]
    since = jnp.zeros((1, value_width), F32)
    for b in range(n):
        ends = expand([ends_out[b, h : h + 1, 0:1] for h in range(heads)], value_width, value_dim)
        before.append(before[-1] + ends)
        since = since + ends * below(b, 2 * z + 2, 2 * n).astype(F32)
    for zz in range(nz):
        reach[zz] = jnp.broadcast_to(
            jnp.exp(jnp.minimum(before[2 * zz] - since, 0.0))
            * below(z, zz, nz).astype(F32),
            (8, value_width),
        )

    def state_ends(b):
        return expand(
            [ends_out[b, h : h + 1, 0:1] for h in range(heads)], value_width, value_dim
        )

    lower = (1 - x).astype(F32)

    key_lane = lax.div(lax.broadcasted_iota(jnp.int32, (tokens, key_width), 1), key_dim)
    value_lane = lax.div(lax.broadcasted_iota(jnp.int32, (tokens, value_width), 1), value_dim)

    def only(values, lane, h):
        return jnp.where(lane == h, values, jnp.zeros_like(values))

    place = lax.broadcasted_iota(jnp.int32, (value_dim, value_width), 0)
    spot = lax.broadcasted_iota(jnp.int32, (value_dim, value_width), 1)
    for h in range(heads):
        put = (place + h * value_dim == spot).astype(F32).astype(BF16)
        incoming[h * key_dim : (h + 1) * key_dim, :] = jnp.dot(
            incoming_ref[0, h].astype(BF16), put, preferred_element_type=F32
        ).astype(BF16)
    for h in range(heads):
        diff = head_total[h] - head_row[h]
        fade[h] = jnp.where(first >= second, jnp.exp(jnp.minimum(diff, 0.0)), 0.0)
        fade_turned[h] = jnp.where(first <= second, jnp.exp(jnp.minimum(-diff, 0.0)), 0.0)
        pointed = lax.dot_general(
            only(key_ref[...], key_lane, h), query_ref[...], across_dims,
            preferred_element_type=F32,
        )
        score[h] = (pointed * fade_turned[h]).astype(BF16)
    for d in range(1, ny):
        outer[d].wait_recv()
        theirs = stream_ref.at[:, columns(lax.rem(y - d + ny, ny) * 2 + c)]
        inner[d] = go(
            remote(theirs, theirs, h_send.at[d], h_recv.at[d], partner), "wait_send"
        )
    band_count = 2 * ny if tokens % (32 * ny) == 0 else 2
    tall = tokens // band_count
    wide = cols_ref.shape[2]
    tp_bands = band_count > 2

    def band(yy, cc):
        return pl.ds(pl.multiple_of((yy * 2 + cc if tp_bands else cc) * tall, tall), tall)

    ret = lax.dot_general(
        stream_ref[:, columns(t)], proj[:, columns(t)], across_dims, preferred_element_type=F32
    )
    for d in range(1, ny):
        tt = lax.rem(y - d + ny, ny) * 2 + c
        ret = ret + lax.dot_general(
            stream_ref[:, columns(tt)], proj[:, columns(tt)], across_dims,
            preferred_element_type=F32,
        )
    for d in range(ny):
        inner[d].wait_recv()

    def piece(b, rows):
        if wide % 128:
            return blocks.at[b, rows]
        return stream_ref.at[rows, pl.ds(pl.multiple_of(b * wide, wide), wide)]

    if wide % 128:
        for b in range(n):
            blocks[b] = stream_ref[:, b * wide : (b + 1) * wide]

    def send_columns(i, e):
        to = member(i, e)
        go(
            remote(
                piece(to, band(y, c)), cols_ref.at[s, band(y, c)],
                c_send.at[2 * i + e], c_recv.at[s], (to, t),
            ),
            "wait_send",
        )

    for i, e in turns:
        send_columns(i, e)
    for d in range(ny):
        tt = lax.rem(y - d + ny, ny) * 2 + 1 - c
        ret = ret + lax.dot_general(
            stream_ref[:, columns(tt)], proj[:, columns(tt)], across_dims,
            preferred_element_type=F32,
        )
    o_ref[...] = ret.astype(BF16)

    injected = lax.dot_general(
        (query_ref[...].astype(F32) * grown).astype(BF16), o_ref[...], along_dims,
        preferred_element_type=F32,
    )
    injected = jnp.where(diagonal, injected, 0.0)
    folded = injected[:key_dim, :]
    for h in range(1, heads):
        folded = folded + injected[h * key_dim : (h + 1) * key_dim, :]
    own_state[...] = folded.astype(BF16)
    pair_copy = go(
        remote(own_state, pair_state, u_send.at[0], u_recv.at[0], (z * 2 + 1 - x, t)),
        "wait_send",
    )
    cols_ref[s] = piece(s, pl.ds(0, tokens))[...]

    query_grad = grown * lax.dot_general(
        o_ref[...], incoming[...], across_dims, preferred_element_type=F32
    )
    key_grad = jnp.zeros((tokens, key_width), F32)
    value_grad = jnp.zeros((tokens, value_width), F32)
    def head_grads(h, grads):
        query_grad, key_grad, value_grad = grads
        o_head = only(o_ref[...], value_lane, h)
        v_head = only(value_ref[...], value_lane, h)
        q_head = only(query_ref[...], key_lane, h)
        k_head = only(key_ref[...], key_lane, h)
        prob = lax.dot_general(o_head, value_ref[...], across_dims, preferred_element_type=F32)
        query_grad = query_grad + jnp.dot(
            (prob * fade[h]).astype(BF16), k_head, preferred_element_type=F32
        )
        prob = lax.dot_general(v_head, o_ref[...], across_dims, preferred_element_type=F32)
        key_grad = key_grad + jnp.dot(
            (prob * fade_turned[h]).astype(BF16), q_head, preferred_element_type=F32
        )
        value_grad = value_grad + jnp.dot(score[h], o_head, preferred_element_type=F32)
        return query_grad, key_grad, value_grad

    from_far, joined = {}, {}

    def columns_arrive(i, e):
        src, k = member(i, e), 2 * i + e
        mine = cols_ref.at[src, band(y, c)]
        remote(
            piece(src, band(y, c)), mine, c_send.at[k], c_recv.at[src], (src, t)
        ).wait_recv()
        if tp_bands:
            for d in range(1, ny):
                from_far[d, k] = go(
                    remote(mine, mine, v_send.at[d, k], v_recv.at[d, k], away(d)), "wait_send"
                )
        joined[0, k] = go(
            remote(mine, mine, w_send.at[0, k], w_recv.at[0, k], partner), "wait_send"
        )

    def columns_relay(i, e):
        src, k = member(i, e), 2 * i + e
        for d in range(1, ny if tp_bands else 1):
            from_far[d, k].wait_recv()
            theirs = cols_ref.at[src, band(lax.rem(y - d + ny, ny), c)]
            joined[d, k] = go(
                remote(theirs, theirs, w_send.at[d, k], w_recv.at[d, k], partner), "wait_send"
            )

    grads = (query_grad, key_grad, value_grad)
    for h in range(heads // 2):
        grads = head_grads(h, grads)
    pair_copy.wait_recv()
    for j in range(2, nz):
        kept_relay(j)
        kept_onward(j)
    mine, other = own_state[...].astype(F32), pair_state[...].astype(F32)
    both = lower * mine + (1.0 - lower) * other + jnp.exp(state_ends(z * 2)) * (
        lower * other + (1.0 - lower) * mine
    )
    both_state[...] = both.astype(BF16)
    for i in range(1, nz):
        go(
            remote(
                both_state, states.at[z], s_send.at[i], s_recv.at[z], (order[i] * 2 + x, t)
            ),
            "wait_send",
        )
    for i, e in turns[:3]:
        columns_arrive(i, e)
    for h in range(heads // 2, heads):
        grads = head_grads(h, grads)
    query_grad, key_grad, value_grad = grads
    query_out[...] = query_grad.astype(BF16)

    def gather(i):
        for e in range(2):
            for d in range(ny if tp_bands else 1):
                if (d, 2 * i + e) in joined:
                    joined[d, 2 * i + e].wait_recv()
        pair = pl.ds(order[i] * 2, 2)
        added = lax.dot_general(
            cols_ref[pair].reshape(2 * tokens, wide),
            kept_out[pair].reshape(2 * tokens, kept_ref.shape[1]),
            along_dims, preferred_element_type=F32,
        )
        if i == 0:
            proj_grad[...] = added
        else:
            proj_grad[...] += added

    for i, e in turns[3:]:
        columns_arrive(i, e)
    for i, e in turns[:3]:
        columns_relay(i, e)
    later = jnp.zeros((key_dim, value_width), F32)
    for i in range(1, nz):
        src = order[i]
        remote(
            both_state, states.at[src], s_send.at[i], s_recv.at[src], (src * 2 + x, t)
        ).wait_recv()
        later = later + reach[src][0:1, :] * states[src].astype(F32)
    for copy in kept_moving:
        copy.wait_recv()
    later = jnp.exp(lower * state_ends(z * 2 + 1)) * later + lower * pair_state[...].astype(F32)
    stacked = jnp.concatenate([later.astype(BF16)] * heads, axis=0)
    stacked = jnp.where(diagonal, stacked, jnp.zeros_like(stacked))
    left = [end - own for end, own in zip(head_end, head_total)]
    key_grad = key_grad + jnp.exp(expand(left, key_width, key_dim)) * lax.dot_general(
        value_ref[...], stacked, across_dims, preferred_element_type=F32
    )
    key_out[...] = key_grad.astype(BF16)
    value_grad = value_grad + jnp.exp(expand(left, value_width, value_dim)) * jnp.dot(
        key_ref[...], stacked, preferred_element_type=F32
    )
    value_out[...] = value_grad.astype(BF16)
    for i, e in turns[3:]:
        columns_relay(i, e)
    for i in range(nz - 1):
        gather(i)
    gather(nz - 1)
    for wait in waits:
        wait()


def main_part(
    n, ny, cap, ids, weights, decay, rows, grad, kept, gate_w, up_w, down_w, proj, query, key,
    value, incoming,
):
    tokens, q = grad.shape
    heads = decay.shape[0]
    dma = pltpu.SemaphoreType.DMA
    slots, model, width = n * cap, rows.shape[1], gate_w.shape[2]
    nz = n // 2
    state = (key.shape[1] // heads, value.shape[1])
    vmem = pl.BlockSpec(memory_space=pltpu.VMEM)
    return pl.pallas_call(
        functools.partial(main_kernel, n, ny, cap),
        out_shape=(
            jax.ShapeDtypeStruct((model // n, kept.shape[1]), F32),
            jax.ShapeDtypeStruct(gate_w.shape, BF16),
            jax.ShapeDtypeStruct(up_w.shape, BF16),
            jax.ShapeDtypeStruct(down_w.shape, BF16),
            jax.ShapeDtypeStruct(query.shape, BF16),
            jax.ShapeDtypeStruct(key.shape, BF16),
            jax.ShapeDtypeStruct(value.shape, BF16),
        ),
        in_specs=[pl.BlockSpec(memory_space=pltpu.HBM)] * 14,
        out_specs=[vmem] * 7,
        scratch_shapes=[
            pltpu.VMEM((n,) + kept.shape, BF16),
            pltpu.VMEM((n, tokens, model // n), BF16),
            pltpu.VMEM((tokens, model), BF16),
            pltpu.VMEM((n, 8, 128), F32),
            pltpu.VMEM(proj.shape, BF16),
            pltpu.VMEM((key.shape[1], value.shape[1]), BF16),
            pltpu.VMEM((tokens, value.shape[1]), BF16),
            pltpu.VMEM((nz,) + state, BF16),
            pltpu.VMEM(state, BF16),
            pltpu.VMEM(state, BF16),
            pltpu.VMEM((nz, 8, value.shape[1]), F32),
            pltpu.VMEM(state, BF16),
            pltpu.VMEM((n, tokens, model // n) if model // n % 128 else (1, 8, 128), BF16),
            pltpu.VMEM((heads, tokens, tokens), F32),
            pltpu.VMEM((heads, tokens, tokens), F32),
            pltpu.VMEM((heads, tokens, tokens), BF16),
            pltpu.VMEM(ids.shape, jnp.int32),
            pltpu.VMEM(weights.shape, F32),
            pltpu.VMEM(decay.shape, F32),
            pltpu.VMEM(grad.shape, BF16),
            pltpu.VMEM(kept.shape, BF16),
            pltpu.VMEM(query.shape, BF16),
            pltpu.VMEM(key.shape, BF16),
            pltpu.VMEM(value.shape, BF16),
            pltpu.VMEM(incoming.shape, F32),
            pltpu.VMEM((tokens, q), BF16),
            pltpu.VMEM(gate_w.shape[1:], BF16),
            pltpu.VMEM(up_w.shape[1:], BF16),
            pltpu.VMEM(down_w.shape[1:], BF16),
            pltpu.VMEM((slots, tokens), BF16),
            pltpu.VMEM((n, 2, cap, q), BF16),
            pltpu.VMEM((2, slots, model), BF16),
            pltpu.VMEM((slots, width), BF16),
            pltpu.VMEM((slots, 2 * width), BF16),
            pltpu.VMEM((slots, model), BF16),
            pltpu.VMEM((ny, slots, q), BF16),
            pltpu.VMEM((ny, slots, q), BF16),
            pltpu.VMEM((ny, slots, q), BF16),
            pltpu.VMEM((slots, q), BF16),
            pltpu.VMEM((slots, q), BF16),
            dma((14,)),
        ]
        + [dma((n,))] * 4
        + [dma((ny, n))] * 4
        + [dma((ny, nz + 1))] * 4
        + [dma((n,))] * 2
        + [dma((ny,))] * 4
        + [dma((n,))] * 6
        + [dma((nz,))] * 2
        + [dma((1,))] * 2
        + [dma((n,))] * 2
        + [dma((ny, n))] * 4,
        compiler_params=pltpu.CompilerParams(
            collective_id=0, has_side_effects=True, vmem_limit_bytes=LIMIT
        ),
    )(
        *(
            pltpu.with_memory_space_constraint(array, pltpu.HBM)
            for array in (
                ids, weights, decay, rows, grad, kept, gate_w, up_w, down_w, proj, query, key,
                value, incoming,
            )
        )
    )


def final_kernel(*refs):
    moved = len(refs) // 2
    copies = [
        pltpu.make_async_copy(source, target, refs[-1].at[j])
        for j, (source, target) in enumerate(zip(refs[:moved], refs[moved:-1]))
    ]
    for copy in copies:
        copy.start()
    for copy in copies:
        copy.wait()


def final_part(*moved):
    return pl.pallas_call(
        final_kernel,
        out_shape=tuple(jax.ShapeDtypeStruct(array.shape, array.dtype) for array in moved),
        in_specs=[pl.BlockSpec(memory_space=pltpu.VMEM)] * len(moved),
        out_specs=[pl.BlockSpec(memory_space=pltpu.HBM)] * len(moved),
        scratch_shapes=[pltpu.SemaphoreType.DMA((len(moved),))],
        compiler_params=pltpu.CompilerParams(vmem_limit_bytes=LIMIT // 4),
    )(*moved)


def on_device(
    moe_input,
    out_grad,
    expert_ids,
    expert_weights,
    w_gate,
    w_up,
    w_down,
    out_proj,
    retained,
    queries,
    keys,
    values,
    log_decay,
    incoming_state,
):
    n, ny = lax.axis_size("sp"), lax.axis_size("tp") // 2
    tokens_here = moe_input.shape[0]
    capacity = -(-(5 * tokens_here // (2 * n)) // 16) * 16
    proj_grad, gate_grad, up_grad, down_grad, query_grad, key_grad, value_grad = final_part(
        *main_part(
            n, ny, capacity, expert_ids.T, expert_weights.T, log_decay.T, moe_input, out_grad,
            retained, w_gate, w_up, w_down, out_proj, queries, keys, values, incoming_state,
        )
    )
    return gate_grad, up_grad, down_grad, proj_grad, query_grad, key_grad, value_grad


def solution(mesh):
    placed = (
        P("sp", None),
        P("sp", "tp"),
        P("sp", None),
        P("sp", None),
        P("sp", None, "tp"),
        P("sp", None, "tp"),
        P("sp", "tp", None),
        P("tp", None),
        P("sp", "tp"),
        P("sp", "tp"),
        P("sp", "tp"),
        P("sp", "tp"),
        P("sp", "tp"),
        P("sp", "tp", None, None),
    )
    return jax.shard_map(
        on_device,
        mesh=mesh,
        in_specs=placed,
        out_specs=(
            P("sp", None, "tp"),
            P("sp", None, "tp"),
            P("sp", "tp", None),
            P("sp", "tp"),
            P("sp", "tp"),
            P("sp", "tp"),
            P("sp", "tp"),
        ),
        check_vma=False,
    )
```

```python
import functools

import jax
import jax.numpy as jnp
from jax import lax
from jax.experimental import pallas as pl
from jax.experimental.pallas import tpu as pltpu
from jax.sharding import PartitionSpec as P

MESH = pl.DeviceIdType.MESH
F32 = jnp.float32
BF16 = jnp.bfloat16
LIMIT = 38 * 1024 * 1024
AHEAD = 5


def where_am_i(n, ny):
    s, t = lax.axis_index("sp"), lax.axis_index("tp")
    return s, t, lax.div(t, 2), lax.rem(t, 2)


def greet(peers):
    barrier = pltpu.get_barrier_semaphore()
    for peer in peers:
        pl.semaphore_signal(barrier, inc=1, device_id=peer, device_id_type=MESH)
    pl.semaphore_wait(barrier, len(peers))


def sp_peers(n, s, t):
    return [(lax.rem(s + k, n), t) for k in range(1, n)]


def tp_peers(ny, s, y, c):
    return [(s, lax.rem(y + d, ny) * 2 + c) for d in range(1, ny)] + [(s, y * 2 + 1 - c)]


def remote(src, dst, send, recv, peer):
    return pltpu.make_async_remote_copy(
        src_ref=src, dst_ref=dst, send_sem=send, recv_sem=recv, device_id=peer, device_id_type=MESH
    )


def below(a, b, top):
    return lax.div(b - a + top - 1, top)


def flipped(z, i, nz):
    if nz & (nz - 1):
        return lax.rem(z + i, nz)
    out, bit = 0, 1
    while bit < nz:
        own = lax.rem(lax.div(z, bit), 2)
        out = out + bit * (1 - own if i & bit else own)
        bit *= 2
    return out


def main_kernel(
    n, ny, cap, ids_hbm, weights_hbm, decay_hbm, rows_hbm, grad_hbm, kept_hbm,
    gate_hbm, up_hbm, down_hbm, proj_hbm, query_hbm, key_hbm, value_hbm, incoming_hbm,
    proj_grad, gate_grad_ref, up_grad_ref, down_grad_ref, query_out, key_out, value_out,
    kept_out, cols_ref, stream_ref, ends_out, proj, incoming, o_ref, states, own_state, pair_state, reach, both_state,

    blocks, fade, fade_turned, score, ids_ref, weights_ref, decay_ref, grad_ref, kept_ref, query_ref, key_ref, value_ref,
    incoming_ref, rows_v, gate_w, up_w, down_w, pick, send, slots, act, both_grads, part, near, pairs, far,
    share, back,
    load_sem, a_send, a_recv, e_send, e_recv, y_send, y_recv, p_send, p_recv,
    n_send, n_recv, f_send, f_recv, b_send, b_recv, g_send, g_recv, h_send, h_recv,
    r_send, r_recv, l_send, l_recv, x_send, x_recv,
    s_send, s_recv, u_send, u_recv, c_send, c_recv, v_send, v_recv, w_send, w_recv,
):
    s, t, y, c = where_am_i(n, ny)
    tokens, q = grad_ref.shape
    heads = decay_ref.shape[0]
    width = gate_w.shape[1]
    nz = n // 2
    z, x = lax.div(s, 2), lax.rem(s, 2)
    partner = (s, y * 2 + 1 - c)
    order = [flipped(z, i, nz) for i in range(nz)]
    waits = []

    def columns(tt):
        return pl.ds(pl.multiple_of(tt * q, q), q)

    def block_rows(b):
        return pl.ds(pl.multiple_of(b * cap, cap), cap)

    def chunk_rows(i):
        return pl.ds(pl.multiple_of(order[i] * 2 * cap, 2 * cap), 2 * cap)

    def member(i, e):
        return order[i] * 2 + (x if e == 0 else 1 - x)

    def away(d):
        return (s, lax.rem(y + d, ny) * 2 + c)

    def go(copy, wait):
        copy.start()
        waits.append(getattr(copy, wait))
        return copy

    barrier = pltpu.get_barrier_semaphore()
    peers = sp_peers(n, s, t) + tp_peers(ny, s, y, c)
    for peer in peers:
        pl.semaphore_signal(barrier, inc=1, device_id=peer, device_id_type=MESH)

    loads = [
        pltpu.make_async_copy(hbm, local, load_sem.at[j])
        for j, (hbm, local) in enumerate(
            [
                (ids_hbm, ids_ref), (weights_hbm, weights_ref), (decay_hbm, decay_ref),
                (grad_hbm, grad_ref), (rows_hbm.at[:, columns(t)], rows_v), (kept_hbm, kept_ref),
                (gate_hbm.at[0], gate_w), (up_hbm.at[0], up_w), (down_hbm.at[0], down_w),
                (proj_hbm, proj), (query_hbm, query_ref), (key_hbm, key_ref),
                (value_hbm, value_ref), (incoming_hbm, incoming_ref),
            ]
        )
    ]
    for copy in loads:
        copy.start()
    for copy in loads[:3]:
        copy.wait()

    ids = ids_ref[...].astype(F32)
    ids = [ids[j : j + 1, :] for j in range(2)]
    weights = [weights_ref[j : j + 1, :] for j in range(2)]
    expert_row = lax.broadcasted_iota(jnp.int32, (n, tokens), 0).astype(F32)
    named = [(expert_row == own).astype(F32) for own in ids]
    first = lax.broadcasted_iota(jnp.int32, (tokens, tokens), 0)
    second = lax.broadcasted_iota(jnp.int32, (tokens, tokens), 1)
    earlier = jnp.dot(
        (named[0] + named[1]).astype(BF16),
        (first < second).astype(F32).astype(BF16),
        preferred_element_type=F32,
    )
    slot = [
        own * cap + jnp.sum(hot * earlier, axis=0, keepdims=True) for own, hot in zip(ids, named)
    ]
    number = lax.broadcasted_iota(jnp.int32, (n * cap, tokens), 0).astype(F32)
    hits = [(number == own).astype(F32) for own in slot]
    picker = (hits[0] + hits[1]).astype(BF16)
    slot_weight = jnp.sum(hits[0] * weights[0] + hits[1] * weights[1], axis=1, keepdims=True)
    pick[...] = picker
    ends_out[s, :, :] = jnp.zeros((8, 128), F32)
    ends_out[s, pl.ds(0, heads), :] = jnp.broadcast_to(
        jnp.sum(decay_ref[...], axis=1, keepdims=True), (heads, 128)
    )
    for copy in loads[3:5]:
        copy.wait()
    cotangent = jnp.dot(picker, grad_ref[...], preferred_element_type=F32) * slot_weight
    send[:, 1] = cotangent.astype(BF16).reshape(n, cap, q)
    picked = jnp.dot(picker, rows_v[...], preferred_element_type=F32).astype(BF16)
    send[:, 0] = picked.reshape(n, cap, q)
    slots[0, block_rows(s), columns(t)] = send[s, 0]
    slots[1, block_rows(s), columns(t)] = send[s, 1]

    pl.semaphore_wait(barrier, len(peers))

    def block(src, tt):
        return slots.at[:, block_rows(src), columns(tt)]

    turns = [(0, 1)]
    for i in range(1, nz - 1, 2):
        turns += [(i, 0), (i + 1, 0), (i, 1), (i + 1, 1)]
    turns += [(nz - 1, 0), (nz - 1, 1)]
    sent = []

    def send_next():
        if len(sent) < len(turns):
            i, e = turns[len(sent)]
            to = member(i, e)
            copy = remote(send.at[to], block(s, t), a_send.at[2 * i + e], a_recv.at[s], (to, t))
            copy.start()
            sent.append(copy)

    for _ in range(AHEAD):
        send_next()

    def at(zz):
        return lax.rem(zz + 2 * nz, nz) * 2 + x

    def hop(j, sign, send_sem, recv_sem, source):
        held = at(z - sign * j)
        return go(
            remote(
                source, kept_out.at[held], send_sem.at[j], recv_sem.at[j], (at(z + sign), t)
            ),
            "wait_send",
        )

    kept_moving = []

    def across(held, index, source):
        kept_moving.append(
            go(
                remote(
                    source, kept_out.at[held], x_send.at[index], x_recv.at[index],
                    (z * 2 + 1 - x, t),
                ),
                "wait_send",
            )
        )

    right_steps, left_steps = nz // 2, nz - 1 - nz // 2
    moving = {}

    def kept_start():
        if right_steps:
            moving["right"] = hop(0, 1, r_send, r_recv, kept_ref)
        if left_steps:
            moving["left"] = hop(0, -1, l_send, l_recv, kept_ref)

    def kept_relay(j):
        if j <= right_steps:
            moving["right"].wait_recv()
            held = at(z - j)
            across(held, 2 * j - 1, kept_out.at[held])
        if j <= left_steps:
            moving["left"].wait_recv()
            held = at(z + j)
            across(held, 2 * j, kept_out.at[held])

    def kept_onward(j):
        if j < right_steps:
            moving["right"] = hop(j, 1, r_send, r_recv, kept_out.at[at(z - j)])
        if j < left_steps:
            moving["left"] = hop(j, -1, l_send, l_recv, kept_out.at[at(z + j)])

    from_far, from_partner = {}, {}

    def arrive(i, e):
        src = member(i, e)
        mine = block(src, t)
        if (i, e) != (0, 0):
            remote(
                send.at[src], mine, a_send.at[2 * i + e], a_recv.at[src], (src, t)
            ).wait_recv()
        k = 2 * i + e
        for d in range(1, ny):
            from_far[d, k] = go(
                remote(mine, mine, y_send.at[d, k], y_recv.at[d, k], away(d)), "wait_send"
            )
        from_partner[0, k] = go(
            remote(mine, mine, p_send.at[0, k], p_recv.at[0, k], partner), "wait_send"
        )
        if k:
            sent[turns.index((i, e))].wait_send()
            send_next()

    def relay(i, e):
        k = 2 * i + e
        for d in range(1, ny):
            from_far[d, k].wait_recv()
            theirs = block(member(i, e), lax.rem(y - d + ny, ny) * 2 + c)
            from_partner[d, k] = go(
                remote(theirs, theirs, p_send.at[d, k], p_recv.at[d, k], partner), "wait_send"
            )

    across_dims = (((1,), (1,)), ((), ()))
    along_dims = (((0,), (0,)), ((), ()))

    units = [(i, None) for i in range(nz - 1)] + [(nz - 1, 0), (nz - 1, 1)]

    def unit_rows(u):
        i, e = units[u]
        return chunk_rows(i) if e is None else block_rows(member(i, e))

    def unit_blocks(u):
        i, e = units[u]
        return [(i, 0), (i, 1)] if e is None else [(i, e)]

    def expert(u):
        for i, e in unit_blocks(u):
            for d in range(ny):
                from_partner[d, 2 * i + e].wait_recv()
        r = unit_rows(u)
        gate = jnp.dot(slots[0, r, :], gate_w[...], preferred_element_type=F32)
        up = jnp.dot(slots[0, r, :], up_w[...], preferred_element_type=F32)
        act_grad = lax.dot_general(
            slots[1, r, :], down_w[...], across_dims, preferred_element_type=F32
        )
        sig = jax.nn.sigmoid(gate)
        swish = gate * sig
        act[r, :] = (swish * up).astype(BF16)
        gate_grad = (act_grad * up * sig * (1.0 + gate * (1.0 - sig))).astype(BF16)
        up_grad = (act_grad * swish).astype(BF16)
        both_grads[r, pl.ds(0, width)] = gate_grad
        both_grads[r, pl.ds(width, width)] = up_grad
        part[r, :] = (
            lax.dot_general(gate_grad, gate_w[...], across_dims, preferred_element_type=F32)
            + lax.dot_general(up_grad, up_w[...], across_dims, preferred_element_type=F32)
        ).astype(BF16)

    halves, summed, returns = {}, {}, {}

    def swap_halves(u):
        r = unit_rows(u)
        for d in list(range(1, ny)) + [0]:
            theirs = lax.rem(y + d, ny) * 2 + 1 - c
            halves[d, u] = go(
                remote(
                    part.at[r, columns(theirs)], near.at[d, r, :],
                    n_send.at[d, u], n_recv.at[d, u], partner,
                ),
                "wait_send",
            )

    def send_pairs(u):
        r = unit_rows(u)
        for d in range(1, ny):
            halves[d, u].wait_recv()
            tt = lax.rem(y + d, ny) * 2 + c
            pairs[d, r, :] = (
                part[r, columns(tt)].astype(F32) + near[d, r, :].astype(F32)
            ).astype(BF16)
            summed[d, u] = go(
                remote(
                    pairs.at[d, r, :], far.at[d, r, :], f_send.at[d, u], f_recv.at[d, u], (s, tt)
                ),
                "wait_send",
            )

    def send_back(u):
        r = unit_rows(u)
        halves[0, u].wait_recv()
        total = part[r, columns(t)].astype(F32) + near[0, r, :].astype(F32)
        for d in range(1, ny):
            summed[d, u].wait_recv()
            total = total + far[d, r, :].astype(F32)
        share[r, :] = total.astype(BF16)
        for i, e in unit_blocks(u):
            to = member(i, e)
            if (i, e) == (0, 0):
                back[block_rows(s), :] = share[block_rows(s), :]
            else:
                go(
                    remote(
                        share.at[block_rows(to), :], back.at[block_rows(s), :],
                        b_send.at[2 * i + e], b_recv.at[s], (to, t),
                    ),
                    "wait_send",
                )

    def returned(i):
        for e in range(2):
            if (i, e) != (0, 0):
                src = member(i, e)
                remote(
                    share.at[block_rows(src), :], back.at[block_rows(src), :],
                    b_send.at[2 * i + e], b_recv.at[src], (src, t),
                ).wait_recv()
        r = chunk_rows(i)
        return lax.dot_general(
            pick[r, :], back[r, :], along_dims, preferred_element_type=F32
        )

    def down_grads():
        turned = act[...].T
        wide = 512
        for j in range(0, down_grad_ref.shape[2], wide):
            down_grad_ref[0, :, j : j + wide] = jnp.dot(
                turned, slots[1, :, j : j + wide], preferred_element_type=F32
            ).astype(BF16)

    def in_grads(lo, hi):
        tall = 256

        def step(j, carry):
            band = pl.ds(pl.multiple_of(j * tall, tall), tall)
            grads = lax.dot_general(
                slots[0, :, band], both_grads[...], along_dims, preferred_element_type=F32
            ).astype(BF16)
            gate_grad_ref[0, band, :] = grads[:, :width]
            up_grad_ref[0, band, :] = grads[:, width:]
            return carry

        count = gate_grad_ref.shape[1] // tall
        lax.fori_loop(lo * count // 4, hi * count // 4, step, 0)

    ends_moving = []
    for k in range(1, n):
        to = lax.rem(s + k, n)
        ends_moving.append(
            go(
                remote(ends_out.at[s], ends_out.at[s], e_send.at[k], e_recv.at[k], (to, t)),
                "wait_send",
            )
        )
    def loaded():
        for copy in loads[5:]:
            copy.wait()

    def forward(i):
        relay(i, 0)
        relay(i, 1)

    def work(u):
        expert(u)
        swap_halves(u)

    arrive(0, 0)
    arrive(0, 1)
    loaded()
    kept_out[s] = kept_ref[...]
    across(s, 0, kept_ref)
    last = nz - 1
    for i in range(1, last, 2):
        arrive(i, 0)
        arrive(i + 1, 0)
        if i == 1:
            forward(0)
        arrive(i, 1)
        if i == 1:
            work(0)
        else:
            forward(i - 1)
            send_pairs(i - 2)
            work(i - 1)
            send_back(i - 3)
        arrive(i + 1, 1)
        forward(i)
        send_pairs(i - 1)
        work(i)
        if i > 1:
            send_back(i - 2)
    arrive(last, 0)
    forward(last - 1)
    arrive(last, 1)
    send_pairs(last - 2)
    kept_start()
    work(last - 1)
    if last > 2:
        send_back(last - 3)
    relay(last, 0)
    send_pairs(last - 1)
    work(last)
    send_back(last - 2)
    relay(last, 1)
    send_pairs(last)
    kept_relay(1)
    send_back(last - 1)
    work(last + 1)
    send_pairs(last + 1)
    send_back(last)
    down_grads()
    send_back(last + 1)
    in_grads(0, 2)
    token = returned(0)
    for i in range(1, nz):
        token = token + returned(i)
    stream_ref[:, columns(t)] = (grad_ref[...].astype(F32) + token).astype(BF16)
    mine = stream_ref.at[:, columns(t)]
    outer = {}
    for d in range(1, ny):
        outer[d] = go(remote(mine, mine, g_send.at[d], g_recv.at[d], away(d)), "wait_send")
    kept_onward(1)
    inner = {}
    inner[0] = go(remote(mine, mine, h_send.at[0], h_recv.at[0], partner), "wait_send")
    in_grads(2, 4)
    value_dim, key_dim = value_ref.shape[1] // heads, key_ref.shape[1] // heads
    def expand(rows, width, depth):
        lane = lax.div(lax.broadcasted_iota(jnp.int32, (rows[0].shape[0], width), 1), depth)
        out = jnp.zeros((rows[0].shape[0], width), F32)
        for h in range(heads):
            out = jnp.where(lane == h, jnp.broadcast_to(rows[h], out.shape), out)
        return out

    key_width, value_width = heads * key_dim, heads * value_dim
    exact = lax.Precision.HIGHEST
    low = (first >= second).astype(F32)
    total = lax.dot_general(
        low, decay_ref[...], across_dims, precision=exact, preferred_element_type=F32
    )
    total_row = lax.dot_general(
        decay_ref[...], low, across_dims, precision=exact, preferred_element_type=F32
    )
    head_total = [total[:, h : h + 1] for h in range(heads)]
    head_row = [total_row[h : h + 1, :] for h in range(heads)]
    head_end = [total[tokens - 1 : tokens, h : h + 1] for h in range(heads)]
    grown = jnp.exp(expand(head_total, key_width, key_dim))
    state_row = lax.div(lax.broadcasted_iota(jnp.int32, (key_width, value_width), 0), key_dim)
    state_lane = lax.div(lax.broadcasted_iota(jnp.int32, (key_width, value_width), 1), value_dim)
    diagonal = state_row == state_lane
    for copy in ends_moving:
        copy.wait_recv()
    before = [jnp.zeros((1, value_width), F32)]
    since = jnp.zeros((1, value_width), F32)
    for b in range(n):
        ends = expand([ends_out[b, h : h + 1, 0:1] for h in range(heads)], value_width, value_dim)
        before.append(before[-1] + ends)
        since = since + ends * below(b, 2 * z + 2, 2 * n).astype(F32)
    for zz in range(nz):
        reach[zz] = jnp.broadcast_to(
            jnp.exp(jnp.minimum(before[2 * zz] - since, 0.0))
            * below(z, zz, nz).astype(F32),
            (8, value_width),
        )

    def state_ends(b):
        return expand(
            [ends_out[b, h : h + 1, 0:1] for h in range(heads)], value_width, value_dim
        )

    lower = (1 - x).astype(F32)

    key_lane = lax.div(lax.broadcasted_iota(jnp.int32, (tokens, key_width), 1), key_dim)
    value_lane = lax.div(lax.broadcasted_iota(jnp.int32, (tokens, value_width), 1), value_dim)

    def only(values, lane, h):
        return jnp.where(lane == h, values, jnp.zeros_like(values))

    place = lax.broadcasted_iota(jnp.int32, (value_dim, value_width), 0)
    spot = lax.broadcasted_iota(jnp.int32, (value_dim, value_width), 1)
    for h in range(heads):
        put = (place + h * value_dim == spot).astype(F32).astype(BF16)
        incoming[h * key_dim : (h + 1) * key_dim, :] = jnp.dot(
            incoming_ref[0, h].astype(BF16), put, preferred_element_type=F32
        ).astype(BF16)
    for h in range(heads):
        diff = head_total[h] - head_row[h]
        fade[h] = jnp.where(first >= second, jnp.exp(jnp.minimum(diff, 0.0)), 0.0)
        fade_turned[h] = jnp.where(first <= second, jnp.exp(jnp.minimum(-diff, 0.0)), 0.0)
        pointed = lax.dot_general(
            only(key_ref[...], key_lane, h), query_ref[...], across_dims,
            preferred_element_type=F32,
        )
        score[h] = (pointed * fade_turned[h]).astype(BF16)
    for d in range(1, ny):
        outer[d].wait_recv()
        theirs = stream_ref.at[:, columns(lax.rem(y - d + ny, ny) * 2 + c)]
        inner[d] = go(
            remote(theirs, theirs, h_send.at[d], h_recv.at[d], partner), "wait_send"
        )
    band_count = 2 * ny if tokens % (32 * ny) == 0 else 2
    tall = tokens // band_count
    wide = cols_ref.shape[2]
    tp_bands = band_count > 2

    def band(yy, cc):
        return pl.ds(pl.multiple_of((yy * 2 + cc if tp_bands else cc) * tall, tall), tall)

    ret = lax.dot_general(
        stream_ref[:, columns(t)], proj[:, columns(t)], across_dims, preferred_element_type=F32
    )
    for d in range(1, ny):
        tt = lax.rem(y - d + ny, ny) * 2 + c
        ret = ret + lax.dot_general(
            stream_ref[:, columns(tt)], proj[:, columns(tt)], across_dims,
            preferred_element_type=F32,
        )
    for d in range(ny):
        inner[d].wait_recv()

    def piece(b, rows):
        if wide % 128:
            return blocks.at[b, rows]
        return stream_ref.at[rows, pl.ds(pl.multiple_of(b * wide, wide), wide)]

    if wide % 128:
        for b in range(n):
            blocks[b] = stream_ref[:, b * wide : (b + 1) * wide]

    def send_columns(i, e):
        to = member(i, e)
        go(
            remote(
                piece(to, band(y, c)), cols_ref.at[s, band(y, c)],
                c_send.at[2 * i + e], c_recv.at[s], (to, t),
            ),
            "wait_send",
        )

    for i, e in turns:
        send_columns(i, e)
    for d in range(ny):
        tt = lax.rem(y - d + ny, ny) * 2 + 1 - c
        ret = ret + lax.dot_general(
            stream_ref[:, columns(tt)], proj[:, columns(tt)], across_dims,
            preferred_element_type=F32,
        )
    o_ref[...] = ret.astype(BF16)

    injected = lax.dot_general(
        (query_ref[...].astype(F32) * grown).astype(BF16), o_ref[...], along_dims,
        preferred_element_type=F32,
    )
    injected = jnp.where(diagonal, injected, 0.0)
    folded = injected[:key_dim, :]
    for h in range(1, heads):
        folded = folded + injected[h * key_dim : (h + 1) * key_dim, :]
    own_state[...] = folded.astype(BF16)
    pair_copy = go(
        remote(own_state, pair_state, u_send.at[0], u_recv.at[0], (z * 2 + 1 - x, t)),
        "wait_send",
    )
    cols_ref[s] = piece(s, pl.ds(0, tokens))[...]

    query_grad = grown * lax.dot_general(
        o_ref[...], incoming[...], across_dims, preferred_element_type=F32
    )
    key_grad = jnp.zeros((tokens, key_width), F32)
    value_grad = jnp.zeros((tokens, value_width), F32)
    def head_grads(h, grads):
        query_grad, key_grad, value_grad = grads
        o_head = only(o_ref[...], value_lane, h)
        v_head = only(value_ref[...], value_lane, h)
        q_head = only(query_ref[...], key_lane, h)
        k_head = only(key_ref[...], key_lane, h)
        prob = lax.dot_general(o_head, value_ref[...], across_dims, preferred_element_type=F32)
        query_grad = query_grad + jnp.dot(
            (prob * fade[h]).astype(BF16), k_head, preferred_element_type=F32
        )
        prob = lax.dot_general(v_head, o_ref[...], across_dims, preferred_element_type=F32)
        key_grad = key_grad + jnp.dot(
            (prob * fade_turned[h]).astype(BF16), q_head, preferred_element_type=F32
        )
        value_grad = value_grad + jnp.dot(score[h], o_head, preferred_element_type=F32)
        return query_grad, key_grad, value_grad

    from_far, joined = {}, {}

    def columns_arrive(i, e):
        src, k = member(i, e), 2 * i + e
        mine = cols_ref.at[src, band(y, c)]
        remote(
            piece(src, band(y, c)), mine, c_send.at[k], c_recv.at[src], (src, t)
        ).wait_recv()
        if tp_bands:
            for d in range(1, ny):
                from_far[d, k] = go(
                    remote(mine, mine, v_send.at[d, k], v_recv.at[d, k], away(d)), "wait_send"
                )
        joined[0, k] = go(
            remote(mine, mine, w_send.at[0, k], w_recv.at[0, k], partner), "wait_send"
        )

    def columns_relay(i, e):
        src, k = member(i, e), 2 * i + e
        for d in range(1, ny if tp_bands else 1):
            from_far[d, k].wait_recv()
            theirs = cols_ref.at[src, band(lax.rem(y - d + ny, ny), c)]
            joined[d, k] = go(
                remote(theirs, theirs, w_send.at[d, k], w_recv.at[d, k], partner), "wait_send"
            )

    grads = (query_grad, key_grad, value_grad)
    for h in range(heads // 2):
        grads = head_grads(h, grads)
    pair_copy.wait_recv()
    for j in range(2, nz):
        kept_relay(j)
        kept_onward(j)
    mine, other = own_state[...].astype(F32), pair_state[...].astype(F32)
    both = lower * mine + (1.0 - lower) * other + jnp.exp(state_ends(z * 2)) * (
        lower * other + (1.0 - lower) * mine
    )
    both_state[...] = both.astype(BF16)
    for i in range(1, nz):
        go(
            remote(
                both_state, states.at[z], s_send.at[i], s_recv.at[z], (order[i] * 2 + x, t)
            ),
            "wait_send",
        )
    for i, e in turns[:3]:
        columns_arrive(i, e)
    for h in range(heads // 2, heads):
        grads = head_grads(h, grads)
    query_grad, key_grad, value_grad = grads
    query_out[...] = query_grad.astype(BF16)

    def gather(i):
        for e in range(2):
            for d in range(ny if tp_bands else 1):
                if (d, 2 * i + e) in joined:
                    joined[d, 2 * i + e].wait_recv()
        pair = pl.ds(order[i] * 2, 2)
        added = lax.dot_general(
            cols_ref[pair].reshape(2 * tokens, wide),
            kept_out[pair].reshape(2 * tokens, kept_ref.shape[1]),
            along_dims, preferred_element_type=F32,
        )
        if i == 0:
            proj_grad[...] = added
        else:
            proj_grad[...] += added

    for i, e in turns[3:]:
        columns_arrive(i, e)
    for i, e in turns[:3]:
        columns_relay(i, e)
    for copy in kept_moving:
        copy.wait_recv()
    gather(0)
    later = jnp.zeros((key_dim, value_width), F32)
    for i in range(1, nz):
        src = order[i]
        remote(
            both_state, states.at[src], s_send.at[i], s_recv.at[src], (src * 2 + x, t)
        ).wait_recv()
        later = later + reach[src][0:1, :] * states[src].astype(F32)
    later = jnp.exp(lower * state_ends(z * 2 + 1)) * later + lower * pair_state[...].astype(F32)
    stacked = jnp.concatenate([later.astype(BF16)] * heads, axis=0)
    stacked = jnp.where(diagonal, stacked, jnp.zeros_like(stacked))
    left = [end - own for end, own in zip(head_end, head_total)]
    key_grad = key_grad + jnp.exp(expand(left, key_width, key_dim)) * lax.dot_general(
        value_ref[...], stacked, across_dims, preferred_element_type=F32
    )
    key_out[...] = key_grad.astype(BF16)
    value_grad = value_grad + jnp.exp(expand(left, value_width, value_dim)) * jnp.dot(
        key_ref[...], stacked, preferred_element_type=F32
    )
    value_out[...] = value_grad.astype(BF16)
    for i, e in turns[3:]:
        columns_relay(i, e)
    for i in range(1, nz - 1):
        gather(i)
    gather(nz - 1)
    for wait in waits:
        wait()


def main_part(
    n, ny, cap, ids, weights, decay, rows, grad, kept, gate_w, up_w, down_w, proj, query, key,
    value, incoming,
):
    tokens, q = grad.shape
    heads = decay.shape[0]
    dma = pltpu.SemaphoreType.DMA
    slots, model, width = n * cap, rows.shape[1], gate_w.shape[2]
    nz = n // 2
    state = (key.shape[1] // heads, value.shape[1])
    vmem = pl.BlockSpec(memory_space=pltpu.VMEM)
    return pl.pallas_call(
        functools.partial(main_kernel, n, ny, cap),
        out_shape=(
            jax.ShapeDtypeStruct((model // n, kept.shape[1]), F32),
            jax.ShapeDtypeStruct(gate_w.shape, BF16),
            jax.ShapeDtypeStruct(up_w.shape, BF16),
            jax.ShapeDtypeStruct(down_w.shape, BF16),
            jax.ShapeDtypeStruct(query.shape, BF16),
            jax.ShapeDtypeStruct(key.shape, BF16),
            jax.ShapeDtypeStruct(value.shape, BF16),
        ),
        in_specs=[pl.BlockSpec(memory_space=pltpu.HBM)] * 14,
        out_specs=[vmem] * 7,
        scratch_shapes=[
            pltpu.VMEM((n,) + kept.shape, BF16),
            pltpu.VMEM((n, tokens, model // n), BF16),
            pltpu.VMEM((tokens, model), BF16),
            pltpu.VMEM((n, 8, 128), F32),
            pltpu.VMEM(proj.shape, BF16),
            pltpu.VMEM((key.shape[1], value.shape[1]), BF16),
            pltpu.VMEM((tokens, value.shape[1]), BF16),
            pltpu.VMEM((nz,) + state, BF16),
            pltpu.VMEM(state, BF16),
            pltpu.VMEM(state, BF16),
            pltpu.VMEM((nz, 8, value.shape[1]), F32),
            pltpu.VMEM(state, BF16),
            pltpu.VMEM((n, tokens, model // n) if model // n % 128 else (1, 8, 128), BF16),
            pltpu.VMEM((heads, tokens, tokens), F32),
            pltpu.VMEM((heads, tokens, tokens), F32),
            pltpu.VMEM((heads, tokens, tokens), BF16),
            pltpu.VMEM(ids.shape, jnp.int32),
            pltpu.VMEM(weights.shape, F32),
            pltpu.VMEM(decay.shape, F32),
            pltpu.VMEM(grad.shape, BF16),
            pltpu.VMEM(kept.shape, BF16),
            pltpu.VMEM(query.shape, BF16),
            pltpu.VMEM(key.shape, BF16),
            pltpu.VMEM(value.shape, BF16),
            pltpu.VMEM(incoming.shape, F32),
            pltpu.VMEM((tokens, q), BF16),
            pltpu.VMEM(gate_w.shape[1:], BF16),
            pltpu.VMEM(up_w.shape[1:], BF16),
            pltpu.VMEM(down_w.shape[1:], BF16),
            pltpu.VMEM((slots, tokens), BF16),
            pltpu.VMEM((n, 2, cap, q), BF16),
            pltpu.VMEM((2, slots, model), BF16),
            pltpu.VMEM((slots, width), BF16),
            pltpu.VMEM((slots, 2 * width), BF16),
            pltpu.VMEM((slots, model), BF16),
            pltpu.VMEM((ny, slots, q), BF16),
            pltpu.VMEM((ny, slots, q), BF16),
            pltpu.VMEM((ny, slots, q), BF16),
            pltpu.VMEM((slots, q), BF16),
            pltpu.VMEM((slots, q), BF16),
            dma((14,)),
        ]
        + [dma((n,))] * 4
        + [dma((ny, n))] * 4
        + [dma((ny, nz + 1))] * 4
        + [dma((n,))] * 2
        + [dma((ny,))] * 4
        + [dma((n,))] * 6
        + [dma((nz,))] * 2
        + [dma((1,))] * 2
        + [dma((n,))] * 2
        + [dma((ny, n))] * 4,
        compiler_params=pltpu.CompilerParams(
            collective_id=0, has_side_effects=True, vmem_limit_bytes=LIMIT
        ),
    )(
        *(
            pltpu.with_memory_space_constraint(array, pltpu.HBM)
            for array in (
                ids, weights, decay, rows, grad, kept, gate_w, up_w, down_w, proj, query, key,
                value, incoming,
            )
        )
    )


def final_kernel(*refs):
    moved = len(refs) // 2
    copies = [
        pltpu.make_async_copy(source, target, refs[-1].at[j])
        for j, (source, target) in enumerate(zip(refs[:moved], refs[moved:-1]))
    ]
    for copy in copies:
        copy.start()
    for copy in copies:
        copy.wait()


def final_part(*moved):
    return pl.pallas_call(
        final_kernel,
        out_shape=tuple(jax.ShapeDtypeStruct(array.shape, array.dtype) for array in moved),
        in_specs=[pl.BlockSpec(memory_space=pltpu.VMEM)] * len(moved),
        out_specs=[pl.BlockSpec(memory_space=pltpu.HBM)] * len(moved),
        scratch_shapes=[pltpu.SemaphoreType.DMA((len(moved),))],
        compiler_params=pltpu.CompilerParams(vmem_limit_bytes=LIMIT // 4),
    )(*moved)


def on_device(
    moe_input,
    out_grad,
    expert_ids,
    expert_weights,
    w_gate,
    w_up,
    w_down,
    out_proj,
    retained,
    queries,
    keys,
    values,
    log_decay,
    incoming_state,
):
    n, ny = lax.axis_size("sp"), lax.axis_size("tp") // 2
    tokens_here = moe_input.shape[0]
    capacity = -(-(5 * tokens_here // (2 * n)) // 16) * 16
    proj_grad, gate_grad, up_grad, down_grad, query_grad, key_grad, value_grad = final_part(
        *main_part(
            n, ny, capacity, expert_ids.T, expert_weights.T, log_decay.T, moe_input, out_grad,
            retained, w_gate, w_up, w_down, out_proj, queries, keys, values, incoming_state,
        )
    )
    return gate_grad, up_grad, down_grad, proj_grad, query_grad, key_grad, value_grad


def solution(mesh):
    placed = (
        P("sp", None),
        P("sp", "tp"),
        P("sp", None),
        P("sp", None),
        P("sp", None, "tp"),
        P("sp", None, "tp"),
        P("sp", "tp", None),
        P("tp", None),
        P("sp", "tp"),
        P("sp", "tp"),
        P("sp", "tp"),
        P("sp", "tp"),
        P("sp", "tp"),
        P("sp", "tp", None, None),
    )
    return jax.shard_map(
        on_device,
        mesh=mesh,
        in_specs=placed,
        out_specs=(
            P("sp", None, "tp"),
            P("sp", None, "tp"),
            P("sp", "tp", None),
            P("sp", "tp"),
            P("sp", "tp"),
            P("sp", "tp"),
            P("sp", "tp"),
        ),
        check_vma=False,
    )
```
